512 devices in a mesh: sp: 32 (over z, core), tp: 16 (over y, x).
Axes of the slice: x: 4, y: 4, z: 16, core: 2. Of those that a mesh axis runs over, the one named last changes fastest.
Arguments:
- residual_in: bfloat16 [8192, 2048], P('sp'), may hold values from -3 to 3
- mix_gain: float32 [2048], replicated, may hold values from 0.1 to 1.9
- pool_weight: bfloat16 [512, 2048], P(None, 'tp'), may hold values from -0.5 to 0.5
- pool_scale: float32 [2048], P('tp'), may hold values from 0.1 to 1.9
- ffn_gain: float32 [2048], replicated, may hold values from 0.1 to 1.9
- route_ids: int32 [8192, 2], P('sp'), may hold values from 0 to 31, all different within a row; in each aligned block of 16 rows (0 to 15, 16 to 31, ...) at most 2 rows name the same one
- route_weights: float32 [8192, 2], P('sp'), may hold values from 0.1 to 1
- gate_weight: bfloat16 [32, 2048, 3584], P('sp', None, 'tp'), may hold values from -0.125 to 0.125
- up_weight: bfloat16 [32, 2048, 3584], P('sp', None, 'tp'), may hold values from -0.125 to 0.125
- down_weight: bfloat16 [32, 3584, 2048], P('sp', 'tp'), may hold values from -0.09375 to 0.09375
Outputs:
- layer_out: bfloat16 [8192, 2048], P('sp')
The draws below stay inside these ranges and needn't reach their ends.
Inputs may be any that keep to these rules, and one draw needn't show every extreme that they name: `route_ids`: each row names 2 different experts; in each aligned block of 16 rows no expert is named by more than 2 rows, and some block has an expert named by exactly 2 rows.
All inputs are finite; a program needn't handle non-finite values.
Results may differ from the reference program's by a relative error of at most 0.0074.
Values may be sent and summed in bfloat16 or wider, within the bound.
A program may use at most 64 MiB of HBM per device.

```python
import math
import jax
import jax.numpy as jnp
import numpy as np
from jax import lax

D = 2048
GROUPS = 4
SPAN = 16
C = 512
FF_EXP = 3584
TOP_K = 2
EXPERTS = 32
ROWS = 16
CAP = 2
TOKENS = 8192
N_TP = 16


def level_of(rng, shape, split, smallest, top_value):
    def one(dim, parts):
        draws = jax.random.uniform(jax.random.fold_in(jax.random.fold_in(rng, 6), dim), (parts,), jnp.float32, smallest / len(split), top_value / len(split))
        return jnp.repeat(jnp.exp(draws), shape[dim] // parts).reshape((-1,) + (1,) * (len(shape) - dim - 1))

    factor_of = one(*split[0])
    for cut in split[1:]:
        factor_of = factor_of * one(*cut)
    return factor_of


def deal_out(key, own, number, rows, number_of, top, most, lean):
    sequence = jax.random.permutation(key, number_of)
    heavy_load, ordinary = shares(number_of, rows * top, most, lean, True), shares(number_of, rows * top, most, lean, False)
    places = jnp.arange(number_of)

    def named(sizes, offset_by):
        used = int((sizes > 0).sum())
        fixed = max(1, used // 4)
        passed = fixed + (places - fixed + offset_by * (used - fixed)) % max(1, number_of - fixed)
        return jnp.zeros((number_of,), jnp.int32).at[sequence[jnp.where(places < fixed, places, passed)]].set(jnp.asarray(sizes, jnp.int32))

    sizes = jnp.where(number % 4 == 0, named(heavy_load, number // 4), named(ordinary, number - number // 4 - 1))
    mixed = jax.random.permutation(jax.random.fold_in(own, 3), number_of)
    source_of, receiver = mixed[0:number_of // 2 * 2:2], mixed[1:number_of // 2 * 2:2]
    room = jnp.minimum(sizes[source_of] - 1, most - sizes[receiver]) // 2
    room = jnp.where((source_of == sequence[0]) | (receiver == sequence[0]) | (sizes[receiver] == 0), 0, jnp.maximum(room, 0))
    passed = jax.random.randint(jax.random.fold_in(own, 4), (number_of // 2,), 0, 1 << 20) % (room + 1)
    sizes = sizes.at[source_of].add(-passed).at[receiver].add(passed)
    items = jnp.searchsorted(jnp.cumsum(sizes), jnp.arange(rows * top), side="right").astype(jnp.int32)
    table = items.reshape(top, rows).T
    table = table[jax.random.permutation(jax.random.fold_in(own, 1), rows)]
    offset_by = jax.random.randint(jax.random.fold_in(own, 2), (rows, 1), 0, top)
    return jnp.take_along_axis(table, (jnp.arange(top)[None, :] + offset_by) % top, axis=1)


def shares(number_of, total, bound, lean, full):
    loads = [(1 << 20) // math.isqrt(standing ** lean) + 1 for standing in range(1, number_of + 1)]
    largest = bound if full else min(bound, max(-(-total // number_of), total * loads[0] // sum(loads)))
    least = 1 if total - largest >= number_of - 1 else 0
    counts, surplus = [largest] + [least] * (number_of - 1), total - largest - least * (number_of - 1)
    while surplus > 0:
        movable = [i for i in range(1, number_of) if counts[i] < largest] or [i for i in range(1, number_of) if counts[i] < bound]
        pool, remaining = sum([loads[i] for i in movable]), surplus
        for i in movable:
            extra = min(bound - counts[i], max(1, remaining * loads[i] // pool), surplus)
            counts[i] = counts[i] + extra
            surplus = surplus - extra
    return np.array(counts)


def gaussian(stream_key, shape, deviation, most, cuts=(), held_as=jnp.bfloat16):
    result = jax.random.normal(stream_key, shape, jnp.float32) * deviation
    if len(cuts) > 0:
        result = level_of(stream_key, shape, cuts, -0.22, 0.18) * result
    return jnp.clip(result, min=-most, max=most).astype(held_as)


def setup_inputs(seed: int = 0) -> dict:
    streams_of = jax.random.split(jax.random.key(seed), 11)
    residual_in = gaussian(streams_of[0], (TOKENS, D), 0.5, 3.0, ((0, 32),))
    mix_gain = jnp.clip(1.0 + 0.18 * jax.random.normal(streams_of[1], (D,), jnp.float32), 0.1, 1.9)
    pool_weight = gaussian(streams_of[2], (C, D), (C // 4) ** -0.5, 0.5, ((1, 16),))
    pool_scale = jnp.clip(1.0 + 0.18 * jax.random.normal(streams_of[3], (D,), jnp.float32), 0.1, 1.9)
    ffn_gain = jnp.clip(1.0 + 0.18 * jax.random.normal(streams_of[4], (D,), jnp.float32), 0.1, 1.9)
    route_ids_keys = jax.random.split(jax.random.fold_in(streams_of[5], 1), TOKENS // ROWS)
    route_ids_turns = jax.random.permutation(jax.random.fold_in(streams_of[5], 3), TOKENS // ROWS)
    route_ids = jax.vmap(lambda own, number: deal_out(jax.random.fold_in(streams_of[5], 2), own, number, ROWS, EXPERTS, TOP_K, CAP, 2))(route_ids_keys, route_ids_turns).reshape((TOKENS, TOP_K))
    route_weights = jnp.clip(jnp.exp(math.log(1.0) - 2.3025851 * jax.random.uniform(streams_of[6], (TOKENS, TOP_K), jnp.float32) ** level_of(streams_of[6], (TOKENS, TOP_K), ((0, 32),), -0.2, 0.2)), 0.1, 1.0)
    gate_weight = gaussian(streams_of[7], (EXPERTS, D, FF_EXP), D ** -0.5, 0.125, ((0, 32), (2, 16)))
    up_weight = gaussian(streams_of[8], (EXPERTS, D, FF_EXP), D ** -0.5, 0.125, ((0, 32), (2, 16)))
    down_weight = gaussian(streams_of[9], (EXPERTS, FF_EXP, D), FF_EXP ** -0.5, 0.09375, ((0, 32), (1, 16)))
    return {"residual_in": residual_in, "mix_gain": mix_gain, "pool_weight": pool_weight, "pool_scale": pool_scale, "ffn_gain": ffn_gain, "route_ids": route_ids, "route_weights": route_weights, "gate_weight": gate_weight, "up_weight": up_weight, "down_weight": down_weight}


EPS = 1e-06

def rms_scale(values, gain):
    return values * lax.rsqrt(lax.optimization_barrier(jnp.mean(values * values, axis=-1, keepdims=True)) + EPS) * gain

def reference(residual_in, mix_gain, pool_weight, pool_scale, ffn_gain, route_ids, route_weights, gate_weight, up_weight, down_weight):
    stream = residual_in.astype(jnp.float32)
    normed_in = rms_scale(stream, mix_gain).astype(jnp.bfloat16)
    shifted_in = jnp.concatenate([jnp.zeros((SPAN, D), jnp.bfloat16), normed_in], axis=0).astype(jnp.float32)
    position = jnp.arange(TOKENS, dtype=jnp.int32)
    pieces = []
    for group_index in range(GROUPS):
        window = 2 ** (group_index + 1)
        first = group_index * C
        window_sum = jnp.zeros((TOKENS, C), jnp.float32)
        for offset in range(window):
            window_sum = window_sum + shifted_in[SPAN - offset:SPAN - offset + TOKENS, first:first + C]
        divisor = jnp.minimum(position + 1, window).astype(jnp.float32)
        pieces.append(window_sum / divisor[:, None] - shifted_in[SPAN:, first:first + C])
    pooled = jnp.concatenate(pieces, axis=1).astype(jnp.bfloat16)
    mapped = jnp.concatenate([jnp.dot(pooled[:, g * C:(g + 1) * C], pool_weight[:, g * C:(g + 1) * C], preferred_element_type=jnp.float32) for g in range(GROUPS)], axis=1)
    mixer_out = (mapped * pool_scale).astype(jnp.bfloat16)
    after_mixer = (stream + mixer_out.astype(jnp.float32)).astype(jnp.bfloat16)
    normed = rms_scale(after_mixer.astype(jnp.float32), ffn_gain).astype(jnp.bfloat16)
    block_count = TOKENS // ROWS
    grouped = route_ids.reshape(block_count, ROWS * TOP_K)
    matches = (grouped[:, :, None] == jnp.arange(EXPERTS, dtype=jnp.int32)[None, None, :]).astype(jnp.int32)
    before = jnp.cumsum(matches, axis=1) - matches
    slot_of = lax.optimization_barrier(jnp.sum(before * matches, axis=-1))
    target = grouped * (block_count * CAP) + jnp.arange(block_count, dtype=jnp.int32)[:, None] * CAP + slot_of
    target = target.reshape(-1).astype(jnp.int32)
    source = (jnp.arange(TOKENS * TOP_K, dtype=jnp.int32) // TOP_K).astype(jnp.int32)
    holder = jnp.zeros((EXPERTS * block_count * CAP,), jnp.int32).at[target].set(source)
    share = FF_EXP // N_TP

    def run_expert(operands):
        indices, gate_matrix, up_matrix, down_matrix = operands
        chosen = normed[indices]
        gate_part = jnp.dot(chosen, gate_matrix, preferred_element_type=jnp.float32)
        up_part = jnp.dot(chosen, up_matrix, preferred_element_type=jnp.float32)
        hidden = (jax.nn.silu(gate_part) * up_part).astype(jnp.bfloat16)
        total = jnp.zeros((indices.shape[0], D), jnp.float32)
        for piece in range(N_TP):
            partial_value = jnp.dot(hidden[:, piece * share:(piece + 1) * share], down_matrix[piece * share:(piece + 1) * share], preferred_element_type=jnp.float32)
            total = total + partial_value.astype(jnp.bfloat16).astype(jnp.float32)
        return total.astype(jnp.bfloat16)
    outputs = lax.map(run_expert, (holder.reshape(EXPERTS, block_count * CAP), gate_weight, up_weight, down_weight))
    picked = outputs.reshape(-1, D)[target].astype(jnp.float32).reshape(TOKENS, TOP_K, D)
    expert_mix = lax.optimization_barrier(jnp.sum(route_weights[:, :, None] * picked, axis=1))
    return (after_mixer.astype(jnp.float32) + expert_mix).astype(jnp.bfloat16)
```

```python
import functools

import jax
import jax.numpy as jnp
from jax import lax
from jax.experimental import pallas as pl
from jax.experimental.pallas import tpu as pltpu
from jax.sharding import Mesh
from jax.sharding import PartitionSpec as P

MESH = pl.DeviceIdType.MESH
AXES = ("z", "c", "y", "x")
EPS = 1e-06
GROUPS = 4
SPAN = 16
NC = 4
STAGES = 9
ORDER = (8, 7, 6, 5, 4, 3, 2, 1, 0)
F32, BF16 = jnp.float32, jnp.bfloat16
NN = (((1,), (0,)), ((), ()))
NT = (((1,), (1,)), ((), ()))


def mm(a, b, dims=NN):
    return lax.dot_general(a, b, dims, preferred_element_type=F32)


def kernel(
    nz,
    res_any, mix_gain, pool_w, pool_scale, ffn_gain, ids, wts, gate_any, up_any, down_any,
    out,
    res, gate, up, down, ng, rim, aft, pick, code, sel, cols,
    sent, slots, part, got1, got2, got3, got4, summed, ret, normed,
    lsem, rim_s, rim_r, dsp_s, dsp_r, ret_s, ret_r, own_s, ag_s, ag_r, rs_s, rs_r, og_s, og_r,
):
    tokens, width = res.shape
    group = width // GROUPS
    experts = nz * 2
    blk = tokens * 2 // 16
    chunk = experts * blk // NC
    half, quart = chunk // 2, chunk // 4
    per = experts // NC
    z, c, y, x = (lax.axis_index(a) for a in AXES)

    def along(axis, d):
        return {axis: ({"x": x, "y": y}[axis] + d) % 4}

    barrier = pltpu.get_barrier_semaphore()
    for r in range(nz):
        for rel in range(2):
            if r or rel:
                pl.semaphore_signal(
                    barrier, 1, device_id={"z": (z + r) % nz, "c": (c + rel) % 2}, device_id_type=MESH
                )
    for axis in ("x", "y"):
        for d in (1, 3):
            pl.semaphore_signal(barrier, 1, device_id=along(axis, d), device_id_type=MESH)

    loads = [
        pltpu.make_async_copy(s, d, lsem.at[i])
        for i, (s, d) in enumerate(((res_any, res), (gate_any, gate), (up_any, up), (down_any, down)))
    ]
    for copy in loads:
        copy.start()

    window = lax.shift_left(jnp.int32(1), y + 1)
    eid = lax.broadcasted_iota(jnp.int32, (experts, tokens), 0)
    m0, m1 = ids[0:1, :] == eid, ids[1:2, :] == eid
    ti = lax.broadcasted_iota(jnp.int32, (tokens, tokens), 0)
    tj = lax.broadcasted_iota(jnp.int32, (tokens, tokens), 1)
    named = jnp.where(m0 | m1, 1.0, 0.0)
    before = mm(named.astype(BF16), jnp.where(ti < tj, 1.0, 0.0).astype(BF16))
    code[...] = jnp.where(m0 | m1, before, -1.0)
    target = eid.astype(F32) * blk + before
    t0 = jnp.sum(jnp.where(m0, target, 0.0), axis=0, keepdims=True)
    t1 = jnp.sum(jnp.where(m1, target, 0.0), axis=0, keepdims=True)
    tall = jnp.concatenate([t0, t1, wts[0:1, :], wts[1:2, :], jnp.zeros((4, tokens), F32)], axis=0)
    cols[...] = jnp.transpose(tall)
    place = lax.broadcasted_iota(jnp.int32, (blk, tokens), 0).astype(F32)
    for e in range(experts):
        pick[e * blk : (e + 1) * blk, :] = jnp.where(code[e : e + 1, :] == place, 1.0, 0.0).astype(BF16)

    loads[0].wait()
    first = pl.multiple_of(y * group, group)
    gain = mix_gain[:, pl.ds(first, group)]
    for b in range(tokens // 32):
        rows = pl.ds(b * 32, 32)
        v = res[rows, :].astype(F32)
        inv = lax.rsqrt(jnp.sum(v * v, axis=1, keepdims=True) / width + EPS)
        ng[rows, :] = (res[rows, pl.ds(first, group)].astype(F32) * inv * gain).astype(BF16)

    pl.semaphore_wait(barrier, nz * 2 + 3)
    nxt = {"z": (z + c) % nz, "c": (c + 1) % 2}
    rim_copy = pltpu.make_async_remote_copy(
        src_ref=ng.at[pl.ds(tokens - SPAN, SPAN)], dst_ref=rim, send_sem=rim_s, recv_sem=rim_r,
        device_id=nxt, device_id_type=MESH,
    )
    rim_copy.start()

    mine = pl.multiple_of((y * 4 + x) * 128, 128)
    start = (z * 2 + c) * tokens

    def mixed_rows(wsum, count):
        pos = start + lax.broadcasted_iota(jnp.int32, (count, 1), 0)
        div = jnp.minimum(pos + 1, window).astype(F32)
        pooled = (wsum / div - ng[0:count, :].astype(F32)).astype(BF16)
        mixed = (mm(pooled, pool_w[...]) * pool_scale[...]).astype(BF16).astype(F32)
        aft[0:count, :] = (res[0:count, pl.ds(mine, 128)].astype(F32) + mixed).astype(BF16)

    band = jnp.where((tj <= ti) & (tj > ti - window), 1.0, 0.0).astype(BF16)
    mixed_rows(mm(band, ng[...]), tokens)

    rim_copy.wait_recv()
    ri = lax.broadcasted_iota(jnp.int32, (SPAN, SPAN), 0)
    rj = lax.broadcasted_iota(jnp.int32, (SPAN, SPAN), 1)
    bend = jnp.where(rj <= ri, jnp.where(rj > ri - window, 1.0, 0.0), 0.0).astype(BF16)
    over = jnp.where(rj - SPAN > ri - window, 1.0, 0.0) * jnp.where(z * 2 + c > 0, 1.0, 0.0)
    mixed_rows(mm(bend, ng[0:SPAN, :]) + mm(over.astype(BF16), rim[...]), SPAN)

    sent[...] = mm(pick[...], aft[...]).astype(BF16)
    for r in range(nz):
        dz = (r + 1) // 2 if r % 2 else -(r // 2)
        for rel in range(2):
            zd, cd = (z - dz + nz) % nz, (c + rel) % 2
            src = sent.at[pl.ds(pl.multiple_of((zd * 2 + cd) * blk, blk), blk)]
            j = 2 * r + rel
            dst = slots.at[y, x, pl.ds(j * blk, blk)]
            if j:
                pltpu.make_async_remote_copy(
                    src_ref=src, dst_ref=dst, send_sem=dsp_s, recv_sem=dsp_r.at[j // per],
                    device_id={"z": zd, "c": cd}, device_id_type=MESH,
                ).start()
            else:
                pltpu.make_async_copy(src, dst, own_s.at[0]).start()

    lane = lax.broadcasted_iota(jnp.int32, (tokens, experts * blk), 1).astype(F32)
    for k in range(2):
        sel[k * tokens : (k + 1) * tokens, :] = jnp.where(cols[:, k : k + 1] == lane, 1.0, 0.0).astype(BF16)

    def landed(ref, sem):
        pltpu.make_async_copy(ref, ref, sem).wait()

    def push(src, dst, s, r, to):
        pltpu.make_async_remote_copy(
            src_ref=src, dst_ref=dst, send_sem=s, recv_sem=r, device_id=to, device_id_type=MESH
        ).start()

    DIRS = ((0, 1), (1, 3))
    HALVES = ((0, "x", "y"), (1, "y", "x"))

    def gather_stages(buf, base_of, hl, qt, ss, rs):
        def rows(k, h, off, n):
            return pl.ds(base_of(k) + h * hl + off, n)

        def one(h, d, k, off, n):
            if h == 0:
                return buf.at[y, (x + d) % 4, rows(k, h, off, n)]
            return buf.at[(y + d) % 4, x, rows(k, h, off, n)]

        def line(h, d, k, off, n):
            if h == 0:
                return buf.at[(y + d) % 4, :, rows(k, h, off, n)]
            return buf.at[:, (x + d) % 4, rows(k, h, off, n)]

        def a1(k):
            for h, ax, _ in HALVES:
                for i, d in DIRS:
                    push(one(h, 0, k, 0, hl), one(h, 0, k, 0, hl), ss.at[k, 0, h, i], rs.at[k, 0, h, i], along(ax, d))

        def a2(k):
            for h, ax, _ in HALVES:
                for i, d in DIRS:
                    landed(one(h, 4 - d, k, 0, hl), rs.at[k, 0, h, i])
                    ref = one(h, 4 - d, k, i * qt, qt)
                    push(ref, ref, ss.at[k, 1, h, i], rs.at[k, 1, h, i], along(ax, d))

        def a3(k):
            for h, _, ax in HALVES:
                for i, d in DIRS:
                    landed(one(h, 2, k, i * qt, qt), rs.at[k, 1, h, i])
                for i, d in DIRS:
                    ref = line(h, 0, k, 0, hl)
                    push(ref, ref, ss.at[k, 2, h, i], rs.at[k, 2, h, i], along(ax, d))

        def a4(k):
            for h, _, ax in HALVES:
                for i, d in DIRS:
                    landed(line(h, 4 - d, k, 0, hl), rs.at[k, 2, h, i])
                    ref = line(h, 4 - d, k, i * qt, qt)
                    push(ref, ref, ss.at[k, 3, h, i], rs.at[k, 3, h, i], along(ax, d))

        def a5(k):
            for h, _, _ in HALVES:
                for i, d in DIRS:
                    landed(line(h, 2, k, i * qt, qt), rs.at[k, 3, h, i])

        def drain(k):
            for h in (0, 1):
                for i in (0, 1):
                    for st, ref in enumerate(
                        (one(h, 0, k, 0, hl), one(h, 0, k, 0, qt), line(h, 0, k, 0, hl), line(h, 0, k, 0, qt))
                    ):
                        landed(ref, ss.at[k, st, h, i])

        return a1, a2, a3, a4, a5, drain

    def base_of(k):
        return pl.multiple_of(k * chunk, chunk)

    a1, a2, a3, a4, a5, ag_drain = gather_stages(slots, base_of, half, quart, ag_s, ag_r)

    def s0(k):
        @pl.when(k == 0)
        def _():
            landed(slots.at[y, x, pl.ds(0, blk)], own_s.at[0])
            landed(slots.at[y, x, pl.ds(blk, chunk - blk)], dsp_r.at[0])

        @pl.when(k > 0)
        def _():
            landed(slots.at[y, x, pl.ds(base_of(k), chunk)], dsp_r.at[k])

        a1(k)

    def line(h, d, k, off, n):
        rows = pl.ds(base_of(k) + h * half + off, n)
        if h == 0:
            return part.at[(y + d) % 4, :, rows]
        return part.at[:, (x + d) % 4, rows]

    def one(h, d, k, off, n):
        rows = pl.ds(base_of(k) + h * half + off, n)
        if h == 0:
            return part.at[y, (x + d) % 4, rows]
        return part.at[(y + d) % 4, x, rows]

    SUMS = ((0, "y", "x"), (1, "x", "y"))

    def ffn(k):
        a5(k)

        @pl.when(k == 0)
        def _():
            for copy in loads[1:]:
                copy.wait()

        def norm(b, carry):
            rows = pl.ds(pl.multiple_of(base_of(k) + b * 32, 32), 32)
            total = jnp.zeros((32, 128), F32)
            for t in range(16):
                v = slots[t // 4, t % 4, rows, :].astype(F32)
                total = total + v * v
            inv = lax.rsqrt(jnp.sum(total, axis=1, keepdims=True) / width + EPS)
            put = pl.ds(pl.multiple_of(b * 32, 32), 32)
            for t in range(16):
                v = slots[t // 4, t % 4, rows, :].astype(F32)
                normed[put, t * 128 : (t + 1) * 128] = (
                    v * inv * ffn_gain[:, t * 128 : (t + 1) * 128]
                ).astype(BF16)
            return carry

        lax.fori_loop(0, chunk // 32, norm, 0)
        g = mm(normed[...], gate[...], NT)
        u = mm(normed[...], up[...], NT)
        hidden = (jax.nn.silu(g) * u).astype(BF16)
        rows = pl.ds(base_of(k), chunk)
        for t in range(0, 16, 2):
            p = mm(hidden, down[:, t * 128 : (t + 2) * 128]).astype(BF16)
            part[t // 4, t % 4, rows, :] = p[:, :128]
            part[t // 4, t % 4 + 1, rows, :] = p[:, 128:]
        for h, ax, _ in SUMS:
            for i, d in DIRS:
                push(line(h, 2, k, i * quart, quart), got1.at[k, h, i], rs_s.at[k, 0, h, i], rs_r.at[k, 0, h, i], along(ax, d))

    def add(ref, *others):
        total = ref[...].astype(F32)
        for other in others:
            total = total + other[...].astype(F32)
        ref[...] = total.astype(BF16)

    def r2(k):
        for h, ax, _ in SUMS:
            for i, d in DIRS:
                landed(got1.at[k, h, i], rs_r.at[k, 0, h, i])
                add(line(h, d, k, i * quart, quart), got1.at[k, h, i])
                push(line(h, d, k, 0, half), got2.at[k, h, i], rs_s.at[k, 1, h, i], rs_r.at[k, 1, h, i], along(ax, d))

    def r3(k):
        for h, _, ax in SUMS:
            for i, d in DIRS:
                landed(got2.at[k, h, i], rs_r.at[k, 1, h, i])
            add(line(h, 0, k, 0, half), got2.at[k, h, 0], got2.at[k, h, 1])
            for i, d in DIRS:
                push(one(h, 2, k, i * quart, quart), got3.at[k, h, i], rs_s.at[k, 2, h, i], rs_r.at[k, 2, h, i], along(ax, d))

    def r4(k):
        for h, _, ax in SUMS:
            for i, d in DIRS:
                landed(got3.at[k, h, i], rs_r.at[k, 2, h, i])
                add(one(h, d, k, i * quart, quart), got3.at[k, h, i])
                push(one(h, d, k, 0, half), got4.at[k, h, i], rs_s.at[k, 3, h, i], rs_r.at[k, 3, h, i], along(ax, d))

    home = pl.ds(pl.multiple_of((z * 2 + c) * blk, blk), blk)

    def back(k):
        for h, _, _ in SUMS:
            for i, d in DIRS:
                landed(got4.at[k, h, i], rs_r.at[k, 3, h, i])
            total = one(h, 0, k, 0, half)[...].astype(F32)
            total = total + got4[k, h, 0].astype(F32) + got4[k, h, 1].astype(F32)
            summed[pl.ds(base_of(k) + h * half, half), :] = total.astype(BF16)
        for i in range(per):
            r = k * (per // 2) + i // 2
            dz = (r % 2) * ((r + 1) // 2) + (1 - r % 2) * (nz - r // 2)
            src = summed.at[pl.ds(pl.multiple_of(base_of(k) + i * blk, blk), blk)]
            to = {"z": (z + dz) % nz, "c": (c + i % 2) % 2}
            if i == 0:

                @pl.when(k == 0)
                def _():
                    pltpu.make_async_copy(src, ret.at[home], own_s.at[1]).start()

                @pl.when(k > 0)
                def _():
                    push(src, ret.at[home], ret_s, ret_r, to)
            else:
                push(src, ret.at[home], ret_s, ret_r, to)

    def rs_drain(k):
        for h in (0, 1):
            for i in (0, 1):
                for st, ref in enumerate((got1, got2, got3, got4)):
                    landed(ref.at[k, h, i], rs_s.at[k, st, h, i])

    stages = (s0, a2, a3, a4, ffn, r2, r3, r4, back)

    def step(tau, carry):
        for s in ORDER:
            k = tau - s

            @pl.when((k >= 0) & (k < NC))
            def _(s=s, k=k):
                stages[s](k)

        return carry

    lax.fori_loop(0, NC + STAGES - 1, step, 0)

    landed(ret.at[pl.ds(0, blk)], own_s.at[1])
    landed(ret.at[pl.ds(blk, (experts - 1) * blk)], ret_r)
    picked = mm(sel[...], ret[...])
    mix = cols[:, 2:3] * picked[:tokens] + cols[:, 3:4] * picked[tokens:]
    out[y, x, :, :] = (aft[...].astype(F32) + mix).astype(BF16)
    o1, o2, o3, o4, o5, og_drain = gather_stages(out, lambda k: 0, tokens // 2, tokens // 4, og_s, og_r)
    for stage in (o1, o2, o3, o4, o5):
        stage(0)

    rim_copy.wait_send()
    landed(sent.at[pl.ds(0, (experts - 1) * blk)], dsp_s)
    landed(summed.at[pl.ds(0, (experts - 1) * blk)], ret_s)

    def drains(k, carry):
        ag_drain(k)
        rs_drain(k)
        return carry

    lax.fori_loop(0, NC, drains, 0)
    og_drain(0)


def shards(res, mix_gain, pool_w, pool_scale, ffn_gain, ids, wts, gate, up, down):
    nz = lax.axis_size("z")
    tokens, width = res.shape
    ff = gate.shape[2]
    experts = nz * 2
    blk = tokens * 2 // 16
    total = experts * blk
    chunk = total // NC
    vmem, hbm = pl.BlockSpec(memory_space=pltpu.VMEM), pl.BlockSpec(memory_space=pl.ANY)
    dma, V = pltpu.SemaphoreType.DMA, pltpu.VMEM
    out = pl.pallas_call(
        functools.partial(kernel, nz),
        name="layer",
        out_shape=jax.ShapeDtypeStruct((4, 4, tokens, 128), BF16),
        in_specs=[hbm, vmem, vmem, vmem, vmem, vmem, vmem, hbm, hbm, hbm],
        out_specs=vmem,
        scratch_shapes=[
            V((tokens, width), BF16),
            V((ff, width), BF16),
            V((ff, width), BF16),
            V((ff, width), BF16),
            V((tokens, width // GROUPS), BF16),
            V((SPAN, width // GROUPS), BF16),
            V((tokens, 128), BF16),
            V((total, tokens), BF16),
            V((experts, tokens), F32),
            V((2 * tokens, total), BF16),
            V((tokens, 8), F32),
            V((total, 128), BF16),
            V((4, 4, total, 128), BF16),
            V((4, 4, total, 128), BF16),
            V((NC, 2, 2, 4, chunk // 4, 128), BF16),
            V((NC, 2, 2, 4, chunk // 2, 128), BF16),
            V((NC, 2, 2, chunk // 4, 128), BF16),
            V((NC, 2, 2, chunk // 2, 128), BF16),
            V((total, 128), BF16),
            V((total, 128), BF16),
            V((chunk, width), BF16),
            dma((4,)),
            dma, dma, dma, dma((NC,)), dma, dma, dma((2,)),
            dma((NC, 4, 2, 2)), dma((NC, 4, 2, 2)), dma((NC, 4, 2, 2)), dma((NC, 4, 2, 2)),
            dma((1, 4, 2, 2)), dma((1, 4, 2, 2)),
        ],
        compiler_params=pltpu.CompilerParams(
            collective_id=0, has_side_effects=True, vmem_limit_bytes=60 * 1024 * 1024
        ),
    )(
        res, mix_gain.reshape(1, -1), pool_w, pool_scale.reshape(1, -1), ffn_gain.reshape(1, -1),
        ids.T, wts.T, gate[0].T, up[0].T, down[0],
    )
    return jnp.transpose(out.reshape(16, tokens, 128), (1, 0, 2)).reshape(tokens, width)


def solution(mesh):
    torus = Mesh(mesh.devices.reshape(mesh.shape["sp"] // 2, 2, 4, 4), AXES)
    sp, tp = ("z", "c"), ("y", "x")
    return jax.shard_map(
        shards,
        mesh=torus,
        in_specs=(
            P(sp, None),
            P(),
            P(None, tp),
            P(tp),
            P(),
            P(sp, None),
            P(sp, None),
            P(sp, None, tp),
            P(sp, None, tp),
            P(sp, tp, None),
        ),
        out_specs=P(sp, None),
        check_vma=False,
    )
```

```python
import functools

import jax
import jax.numpy as jnp
from jax import lax
from jax.experimental import pallas as pl
from jax.experimental.pallas import tpu as pltpu
from jax.sharding import Mesh
from jax.sharding import PartitionSpec as P

MESH = pl.DeviceIdType.MESH
AXES = ("z", "c", "y", "x")
EPS = 1e-06
GROUPS = 4
SPAN = 16
NC = 4
ORDER = (0, 1, 2, 3, 4, 5, 6)
NO = 2
DZ = (0, 1, -1, 2, -4, 5, -5, 6, -6, 7, -7, 8, -2, 3, -3, 4)
TOKENS = True
SPLIT = 2
F32, BF16 = jnp.float32, jnp.bfloat16
NN = (((1,), (0,)), ((), ()))
NT = (((1,), (1,)), ((), ()))


def mm(a, b, dims=NN):
    return lax.dot_general(a, b, dims, preferred_element_type=F32)


def kernel(
    nz,
    res_any, mix_gain, pool_w, pool_scale, ffn_gain, ids, wts, gate_any, up_any, down_any,
    out_any,
    res, gate, up, down, ng, rim, aft, pick, code, sel, cols,
    sent, slots, part, got1, got2, got3, summed, ret, normed, out,
    lsem, rim_s, rim_r, dsp_s, dsp_r, ret_s, ret_r, own_s, ag_s, ag_r, rs_s, rs_r, og_s, og_r, out_s, tokp, tokm,
):
    tokens, width = res.shape
    group = width // GROUPS
    experts = nz * 2
    blk = tokens * 2 // 16
    chunk = experts * blk // NC
    half, quart = chunk // 2, chunk // 4
    per = experts // NC
    z, c, y, x = (lax.axis_index(a) for a in AXES)

    def along(axis, d):
        return {axis: ({"x": x, "y": y}[axis] + d) % 4}

    barrier = pltpu.get_barrier_semaphore()
    reach = (0, 1, nz - 1) if TOKENS else range(nz)
    for r in reach:
        for rel in range(2):
            if r or rel:
                pl.semaphore_signal(
                    barrier, 1, device_id={"z": (z + r) % nz, "c": (c + rel) % 2}, device_id_type=MESH
                )
    for axis in ("x", "y"):
        for d in (1, 2, 3):
            pl.semaphore_signal(barrier, 1, device_id=along(axis, d), device_id_type=MESH)

    loads = [
        pltpu.make_async_copy(s, d, lsem.at[i])
        for i, (s, d) in enumerate(((res_any, res), (gate_any, gate), (up_any, up), (down_any, down)))
    ]
    for copy in loads:
        copy.start()

    def pass_on(h):
        if not TOKENS:
            return
        if h > 1:
            pl.semaphore_wait(tokp.at[h], 1)
            if h < nz // 2:
                pl.semaphore_wait(tokm.at[h], 1)
        if h < nz // 2:
            pl.semaphore_signal(tokp.at[h + 1], 1, device_id={"z": (z + 1) % nz}, device_id_type=MESH)
        if h < nz // 2 - 1:
            pl.semaphore_signal(tokm.at[h + 1], 1, device_id={"z": (z + nz - 1) % nz}, device_id_type=MESH)

    window = lax.shift_left(jnp.int32(1), y + 1)
    first = pl.multiple_of(y * group, group)
    gain = mix_gain[:, pl.ds(first, group)]

    def norm_rows(at, n):
        rows = pl.ds(at, n)
        v = res[rows, :].astype(F32)
        inv = lax.rsqrt(jnp.sum(v * v, axis=1, keepdims=True) / width + EPS)
        ng[rows, :] = (res[rows, pl.ds(first, group)].astype(F32) * inv * gain).astype(BF16)

    eid = lax.broadcasted_iota(jnp.int32, (experts, tokens), 0)
    m0, m1 = ids[0:1, :] == eid, ids[1:2, :] == eid
    ti = lax.broadcasted_iota(jnp.int32, (tokens, tokens), 0)
    tj = lax.broadcasted_iota(jnp.int32, (tokens, tokens), 1)
    named = jnp.where(m0 | m1, 1.0, 0.0)
    before = mm(named.astype(BF16), jnp.where(ti < tj, 1.0, 0.0).astype(BF16))
    code[...] = jnp.where(m0 | m1, before, -1.0)
    target = eid.astype(F32) * blk + before
    t0 = jnp.sum(jnp.where(m0, target, 0.0), axis=0, keepdims=True)
    t1 = jnp.sum(jnp.where(m1, target, 0.0), axis=0, keepdims=True)
    tall = jnp.concatenate([t0, t1, wts[0:1, :], wts[1:2, :], jnp.zeros((4, tokens), F32)], axis=0)
    cols[...] = jnp.transpose(tall)
    place = lax.broadcasted_iota(jnp.int32, (blk, tokens), 0).astype(F32)

    loads[0].wait()
    norm_rows(tokens - 32, 32)
    pl.semaphore_wait(barrier, 11 if TOKENS else nz * 2 + 5)
    nxt = {"z": (z + c) % nz, "c": (c + 1) % 2}
    rim_copy = pltpu.make_async_remote_copy(
        src_ref=ng.at[pl.ds(tokens - SPAN, SPAN)], dst_ref=rim, send_sem=rim_s, recv_sem=rim_r,
        device_id=nxt, device_id_type=MESH,
    )
    rim_copy.start()
    pass_on(1)

    for b in range(tokens // 32 - 1):
        norm_rows(b * 32, 32)
    pass_on(2)

    mine = pl.multiple_of((y * 4 + x) * 128, 128)
    start = (z * 2 + c) * tokens

    def mixed_rows(wsum, count):
        pos = start + lax.broadcasted_iota(jnp.int32, (count, 1), 0)
        div = jnp.minimum(pos + 1, window).astype(F32)
        pooled = (wsum / div - ng[0:count, :].astype(F32)).astype(BF16)
        mixed = (mm(pooled, pool_w[...]) * pool_scale[...]).astype(BF16).astype(F32)
        aft[0:count, :] = (res[0:count, pl.ds(mine, 128)].astype(F32) + mixed).astype(BF16)

    band = jnp.where((tj <= ti) & (tj > ti - window), 1.0, 0.0).astype(BF16)
    mixed_rows(mm(band, ng[...]), tokens)
    for e in range(experts):
        pick[e * blk : (e + 1) * blk, :] = jnp.where(code[e : e + 1, :] == place, 1.0, 0.0).astype(BF16)
    pass_on(3)

    rim_copy.wait_recv()
    ri = lax.broadcasted_iota(jnp.int32, (SPAN, SPAN), 0)
    rj = lax.broadcasted_iota(jnp.int32, (SPAN, SPAN), 1)
    bend = jnp.where(rj <= ri, jnp.where(rj > ri - window, 1.0, 0.0), 0.0).astype(BF16)
    over = jnp.where(rj - SPAN > ri - window, 1.0, 0.0) * jnp.where(z * 2 + c > 0, 1.0, 0.0)
    mixed_rows(mm(bend, ng[0:SPAN, :]) + mm(over.astype(BF16), rim[...]), SPAN)

    sent[...] = mm(pick[...], aft[...]).astype(BF16)
    known = 3
    for r, dz in enumerate(DZ):
        while known < abs(dz):
            known += 1
            pass_on(known)
        for rel in range(2):
            zd, cd = (z + (nz - dz) % nz) % nz, (c + rel) % 2
            src = sent.at[pl.ds(pl.multiple_of((zd * 2 + cd) * blk, blk), blk)]
            j = 2 * r + rel
            dst = slots.at[y, x, pl.ds(j * blk, blk)]
            if j:
                pltpu.make_async_remote_copy(
                    src_ref=src, dst_ref=dst, send_sem=dsp_s, recv_sem=dsp_r.at[j // per],
                    device_id={"z": zd, "c": cd}, device_id_type=MESH,
                ).start()
            else:
                pltpu.make_async_copy(src, dst, own_s.at[0]).start()

    lane = lax.broadcasted_iota(jnp.int32, (tokens, experts * blk), 1).astype(F32)
    for k in range(2):
        sel[k * tokens : (k + 1) * tokens, :] = jnp.where(cols[:, k : k + 1] == lane, 1.0, 0.0).astype(BF16)

    def landed(ref, sem):
        pltpu.make_async_copy(ref, ref, sem).wait()

    def push(src, dst, s, r, to):
        pltpu.make_async_remote_copy(
            src_ref=src, dst_ref=dst, send_sem=s, recv_sem=r, device_id=to, device_id_type=MESH
        ).start()

    DIRS = ((0, 1), (1, 3))
    HALVES = ((0, "x", "y"), (1, "y", "x"))

    def pieces(hl):
        cut = hl * SPLIT // 4
        return ((0, 1, 0, cut), (1, 3, cut, hl - cut))

    def gather_stages(buf, base_of, hl, ss, rs):
        def rows(k, h, off, n):
            return pl.ds(base_of(k) + h * hl + off, n)

        def one(h, d, k, off, n):
            if h == 0:
                return buf.at[y, (x + d) % 4, rows(k, h, off, n)]
            return buf.at[(y + d) % 4, x, rows(k, h, off, n)]

        def line(h, d, k, off, n):
            if h == 0:
                return buf.at[(y + d) % 4, :, rows(k, h, off, n)]
            return buf.at[:, (x + d) % 4, rows(k, h, off, n)]

        def a1(k):
            for d in (1, 3, 2):
                for h, ax, _ in HALVES:
                    push(one(h, 0, k, 0, hl), one(h, 0, k, 0, hl), ss.at[k, 0, h, d - 1], rs.at[k, 0, h, d - 1], along(ax, d))

        def a2(k):
            for h, _, ax in HALVES:
                for d in (1, 3, 2):
                    landed(one(h, 4 - d, k, 0, hl), rs.at[k, 0, h, d - 1])
                for i, d in DIRS:
                    ref = line(h, 0, k, 0, hl)
                    push(ref, ref, ss.at[k, 1, h, i], rs.at[k, 1, h, i], along(ax, d))

        def a3(k):
            for h, _, ax in HALVES:
                for i, d, off, n in pieces(hl):
                    landed(line(h, 4 - d, k, 0, hl), rs.at[k, 1, h, i])
                    ref = line(h, 4 - d, k, off, n)
                    push(ref, ref, ss.at[k, 2, h, i], rs.at[k, 2, h, i], along(ax, d))

        def a4(k):
            for h, _, _ in HALVES:
                for i, d, off, n in pieces(hl):
                    landed(line(h, 2, k, off, n), rs.at[k, 2, h, i])

        def drain(k):
            for h in (0, 1):
                for d in (1, 2, 3):
                    landed(one(h, 0, k, 0, hl), ss.at[k, 0, h, d - 1])
                for i, _, off, n in pieces(hl):
                    landed(line(h, 0, k, 0, hl), ss.at[k, 1, h, i])
                    landed(line(h, 0, k, 0, n), ss.at[k, 2, h, i])

        return a1, a2, a3, a4, drain

    def base_of(k):
        return pl.multiple_of(k * chunk, chunk)

    a1, a2, a3, a4, ag_drain = gather_stages(slots, base_of, half, ag_s, ag_r)

    def s0(k):
        @pl.when(k == 0)
        def _():
            landed(slots.at[y, x, pl.ds(0, blk)], own_s.at[0])
            landed(slots.at[y, x, pl.ds(blk, chunk - blk)], dsp_r.at[0])

        @pl.when(k > 0)
        def _():
            landed(slots.at[y, x, pl.ds(base_of(k), chunk)], dsp_r.at[k])

        a1(k)

    def line(h, d, k, off, n):
        rows = pl.ds(base_of(k) + h * half + off, n)
        if h == 0:
            return part.at[(y + d) % 4, :, rows]
        return part.at[:, (x + d) % 4, rows]

    def one(h, d, k, off, n):
        rows = pl.ds(base_of(k) + h * half + off, n)
        if h == 0:
            return part.at[y, (x + d) % 4, rows]
        return part.at[(y + d) % 4, x, rows]

    SUMS = ((0, "y", "x"), (1, "x", "y"))

    def ffn(k):
        a4(k)

        @pl.when(k == 0)
        def _():
            for copy in loads[1:]:
                copy.wait()

        def norm(b, carry):
            rows = pl.ds(pl.multiple_of(base_of(k) + b * 32, 32), 32)
            total = jnp.zeros((32, 128), F32)
            for t in range(16):
                v = slots[t // 4, t % 4, rows, :].astype(F32)
                total = total + v * v
            inv = lax.rsqrt(jnp.sum(total, axis=1, keepdims=True) / width + EPS)
            put = pl.ds(pl.multiple_of(b * 32, 32), 32)
            for t in range(16):
                v = slots[t // 4, t % 4, rows, :].astype(F32)
                normed[put, t * 128 : (t + 1) * 128] = (
                    v * inv * ffn_gain[:, t * 128 : (t + 1) * 128]
                ).astype(BF16)
            return carry

        lax.fori_loop(0, chunk // 32, norm, 0)
        g = mm(normed[...], gate[...], NT)
        u = mm(normed[...], up[...], NT)
        hidden = (jax.nn.silu(g) * u).astype(BF16)
        rows = pl.ds(base_of(k), chunk)
        for t in range(0, 16, 2):
            p = mm(hidden, down[:, t * 128 : (t + 2) * 128]).astype(BF16)
            part[t // 4, t % 4, rows, :] = p[:, :128]
            part[t // 4, t % 4 + 1, rows, :] = p[:, 128:]
        for h, ax, _ in SUMS:
            for i, d, off, n in pieces(half):
                push(line(h, 2, k, off, n), got1.at[k, h, :, pl.ds(off, n)], rs_s.at[k, 0, h, i], rs_r.at[k, 0, h, i], along(ax, d))

    def add(ref, *others):
        total = ref[...].astype(F32)
        for other in others:
            total = total + other[...].astype(F32)
        ref[...] = total.astype(BF16)

    def r2(k):
        for h, ax, _ in SUMS:
            for i, d, off, n in pieces(half):
                landed(got1.at[k, h, :, pl.ds(off, n)], rs_r.at[k, 0, h, i])
                add(line(h, d, k, off, n), got1.at[k, h, :, pl.ds(off, n)])
                push(line(h, d, k, 0, half), got2.at[k, h, i], rs_s.at[k, 1, h, i], rs_r.at[k, 1, h, i], along(ax, d))

    def r3(k):
        for h, _, ax in SUMS:
            for i, d in DIRS:
                landed(got2.at[k, h, i], rs_r.at[k, 1, h, i])
            add(line(h, 0, k, 0, half), got2.at[k, h, 0], got2.at[k, h, 1])
            for d in (2, 1, 3):
                push(one(h, d, k, 0, half), got3.at[k, h, d - 1], rs_s.at[k, 2, h, d - 1], rs_r.at[k, 2, h, d - 1], along(ax, d))

    home = pl.ds(pl.multiple_of((z * 2 + c) * blk, blk), blk)

    def back(k):
        for h, _, _ in SUMS:
            for d in (1, 3, 2):
                landed(got3.at[k, h, d - 1], rs_r.at[k, 2, h, d - 1])
            total = one(h, 0, k, 0, half)[...].astype(F32)
            for d in (1, 2, 3):
                total = total + got3[k, h, d - 1].astype(F32)
            summed[pl.ds(base_of(k) + h * half, half), :] = total.astype(BF16)
        for kk in range(NC):

            @pl.when(k == kk)
            def _(kk=kk):
                for i in range(per):
                    j = kk * per + i
                    src = summed.at[pl.ds(j * blk, blk)]
                    to = {"z": (z + (DZ[j // 2] + nz) % nz) % nz, "c": (c + j % 2) % 2}
                    if j:
                        push(src, ret.at[home], ret_s, ret_r, to)
                    else:
                        pltpu.make_async_copy(src, ret.at[home], own_s.at[1]).start()

    def rs_drain(k):
        for h in (0, 1):
            for i, _, off, n in pieces(half):
                landed(got1.at[k, h, :, pl.ds(off, n)], rs_s.at[k, 0, h, i])
                landed(got2.at[k, h, i], rs_s.at[k, 1, h, i])
            for d in (1, 2, 3):
                landed(got3.at[k, h, d - 1], rs_s.at[k, 2, h, d - 1])

    stages = (s0, a2, a3, ffn, r2, r3, back)

    def step(tau, carry):
        for s in ORDER:
            k = tau - s

            @pl.when((k >= 0) & (k < NC))
            def _(s=s, k=k):
                stages[s](k)

        return carry

    lax.fori_loop(0, NC + len(stages) - 1, step, 0)

    landed(ret.at[pl.ds(0, blk)], own_s.at[1])
    landed(ret.at[pl.ds(blk, (experts - 1) * blk)], ret_r)
    picked = mm(sel[...], ret[...])
    mix = cols[:, 2:3] * picked[:tokens] + cols[:, 3:4] * picked[tokens:]
    out[y, x, :, :] = (aft[...].astype(F32) + mix).astype(BF16)
    oc = tokens // NO
    *over_out, og_drain = gather_stages(out, lambda k: k * oc, oc // 2, og_s, og_r)
    for tau in range(NO + 3):
        for s, stage in enumerate(over_out):
            if 0 <= tau - s < NO:
                stage(tau - s)
    puts = [
        pltpu.make_async_copy(out.at[t // 4, t % 4], out_any.at[:, pl.ds(t * 128, 128)], out_s.at[t])
        for t in range(16)
    ]
    for copy in puts:
        copy.start()

    rim_copy.wait_send()
    landed(sent.at[pl.ds(0, (experts - 1) * blk)], dsp_s)
    landed(summed.at[pl.ds(0, (experts - 1) * blk)], ret_s)

    def drains(k, carry):
        ag_drain(k)
        rs_drain(k)
        return carry

    lax.fori_loop(0, NC, drains, 0)
    for k in range(NO):
        og_drain(k)
    for copy in puts:
        copy.wait()


def shards(res, mix_gain, pool_w, pool_scale, ffn_gain, ids, wts, gate, up, down):
    nz = lax.axis_size("z")
    tokens, width = res.shape
    ff = gate.shape[2]
    experts = nz * 2
    blk = tokens * 2 // 16
    total = experts * blk
    chunk = total // NC
    vmem, hbm = pl.BlockSpec(memory_space=pltpu.VMEM), pl.BlockSpec(memory_space=pl.ANY)
    dma, V = pltpu.SemaphoreType.DMA, pltpu.VMEM
    out = pl.pallas_call(
        functools.partial(kernel, nz),
        name="layer",
        out_shape=jax.ShapeDtypeStruct((tokens, width), BF16),
        in_specs=[hbm, vmem, vmem, vmem, vmem, vmem, vmem, hbm, hbm, hbm],
        out_specs=hbm,
        scratch_shapes=[
            V((tokens, width), BF16),
            V((ff, width), BF16),
            V((ff, width), BF16),
            V((ff, width), BF16),
            V((tokens, width // GROUPS), BF16),
            V((SPAN, width // GROUPS), BF16),
            V((tokens, 128), BF16),
            V((total, tokens), BF16),
            V((experts, tokens), F32),
            V((2 * tokens, total), BF16),
            V((tokens, 8), F32),
            V((total, 128), BF16),
            V((4, 4, total, 128), BF16),
            V((4, 4, total, 128), BF16),
            V((NC, 2, 4, chunk // 2, 128), BF16),
            V((NC, 2, 2, 4, chunk // 2, 128), BF16),
            V((NC, 2, 3, chunk // 2, 128), BF16),
            V((total, 128), BF16),
            V((total, 128), BF16),
            V((chunk, width), BF16),
            V((4, 4, tokens, 128), BF16),
            dma((4,)),
            dma, dma, dma, dma((NC,)), dma, dma, dma((2,)),
            dma((NC, 3, 2, 3)), dma((NC, 3, 2, 3)), dma((NC, 3, 2, 3)), dma((NC, 3, 2, 3)),
            dma((NO, 3, 2, 3)), dma((NO, 3, 2, 3)), dma((16,)),
            pltpu.SemaphoreType.REGULAR((9,)), pltpu.SemaphoreType.REGULAR((9,)),
        ],
        compiler_params=pltpu.CompilerParams(
            collective_id=0, has_side_effects=True, vmem_limit_bytes=60 * 1024 * 1024
        ),
    )(
        res, mix_gain.reshape(1, -1), pool_w, pool_scale.reshape(1, -1), ffn_gain.reshape(1, -1),
        ids.T, wts.T, gate[0].T, up[0].T, down[0],
    )
    return out


def solution(mesh):
    torus = Mesh(mesh.devices.reshape(mesh.shape["sp"] // 2, 2, 4, 4), AXES)
    sp, tp = ("z", "c"), ("y", "x")
    return jax.shard_map(
        shards,
        mesh=torus,
        in_specs=(
            P(sp, None),
            P(),
            P(None, tp),
            P(tp),
            P(),
            P(sp, None),
            P(sp, None),
            P(sp, None, tp),
            P(sp, None, tp),
            P(sp, tp, None),
        ),
        out_specs=P(sp, None),
        check_vma=False,
    )
```

```python
import functools

import jax
import jax.numpy as jnp
from jax import lax
from jax.experimental import pallas as pl
from jax.experimental.pallas import tpu as pltpu
from jax.sharding import Mesh
from jax.sharding import PartitionSpec as P

MESH = pl.DeviceIdType.MESH
AXES = ("z", "c", "y", "x")
EPS = 1e-06
GROUPS = 4
SPAN = 16
NC = 4
ORDER = (2, 1, 0, 3, 4, 5, 6)
NO = 2
DZ = (0, 1, -1, 2, -2, 3, -3, 4, -6, 7, -7, 8, -4, 5, -5, 6)
SPLIT = 2
F32, BF16 = jnp.float32, jnp.bfloat16
NN = (((1,), (0,)), ((), ()))
NT = (((1,), (1,)), ((), ()))


def mm(a, b, dims=NN):
    return lax.dot_general(a, b, dims, preferred_element_type=F32)


def kernel(
    nz,
    res_any, mix_gain, pool_w, pool_scale, ffn_gain, ids, wts, gate_any, up_any, down_any,
    out,
    res, gate, up, down, ng, rim, aft, pick, code, sel, cols,
    sent, slots, part, got1, got2, got3, summed, ret, normed,
    lsem, rim_s, rim_r, dsp_s, dsp_r, ret_s, ret_r, own_s, ag_s, ag_r, rs_s, rs_r, og_s, og_r, tok,
):
    tokens, width = res.shape
    group = width // GROUPS
    experts = nz * 2
    blk = tokens * 2 // 16
    chunk = experts * blk // NC
    half, quart = chunk // 2, chunk // 4
    per = experts // NC
    z, c, y, x = (lax.axis_index(a) for a in AXES)

    def along(axis, d):
        return {axis: ({"x": x, "y": y}[axis] + d) % 4}

    loads = [
        pltpu.make_async_copy(s, d, lsem.at[i])
        for i, (s, d) in enumerate(((res_any, res), (gate_any, gate), (up_any, up), (down_any, down)))
    ]
    for copy in loads:
        copy.start()

    barrier = pltpu.get_barrier_semaphore()
    for r in (0, 1, 2, nz - 2, nz - 1):
        for rel in range(2):
            if r or rel:
                pl.semaphore_signal(
                    barrier, 1, device_id={"z": (z + r) % nz, "c": (c + rel) % 2}, device_id_type=MESH
                )
    for axis in ("x", "y"):
        for d in (1, 2, 3):
            pl.semaphore_signal(barrier, 1, device_id=along(axis, d), device_id_type=MESH)

    def tell(r):
        for d in (r, nz - r):
            pl.semaphore_signal(tok.at[r // 4], 1, device_id={"z": (z + d) % nz}, device_id_type=MESH)

    def told(r):
        pl.semaphore_wait(tok.at[r // 4], 2)

    window = lax.shift_left(jnp.int32(1), y + 1)
    first = pl.multiple_of(y * group, group)
    gain = mix_gain[:, pl.ds(first, group)]

    def norm_rows(at, n):
        rows = pl.ds(at, n)
        v = res[rows, :].astype(F32)
        inv = lax.rsqrt(jnp.sum(v * v, axis=1, keepdims=True) / width + EPS)
        ng[rows, :] = (res[rows, pl.ds(first, group)].astype(F32) * inv * gain).astype(BF16)

    eid = lax.broadcasted_iota(jnp.int32, (experts, tokens), 0)
    m0, m1 = ids[0:1, :] == eid, ids[1:2, :] == eid
    ti = lax.broadcasted_iota(jnp.int32, (tokens, tokens), 0)
    tj = lax.broadcasted_iota(jnp.int32, (tokens, tokens), 1)
    named = jnp.where(m0 | m1, 1.0, 0.0)
    before = mm(named.astype(BF16), jnp.where(ti < tj, 1.0, 0.0).astype(BF16))
    code[...] = jnp.where(m0 | m1, before, -1.0)
    target = eid.astype(F32) * blk + before
    t0 = jnp.sum(jnp.where(m0, target, 0.0), axis=0, keepdims=True)
    t1 = jnp.sum(jnp.where(m1, target, 0.0), axis=0, keepdims=True)
    tall = jnp.concatenate([t0, t1, wts[0:1, :], wts[1:2, :], jnp.zeros((4, tokens), F32)], axis=0)
    cols[...] = jnp.transpose(tall)
    place = lax.broadcasted_iota(jnp.int32, (blk, tokens), 0).astype(F32)

    loads[0].wait()
    norm_rows(tokens - 32, 32)
    pl.semaphore_wait(barrier, 15)
    nxt = {"z": (z + c) % nz, "c": (c + 1) % 2}
    rim_copy = pltpu.make_async_remote_copy(
        src_ref=ng.at[pl.ds(tokens - SPAN, SPAN)], dst_ref=rim, send_sem=rim_s, recv_sem=rim_r,
        device_id=nxt, device_id_type=MESH,
    )
    rim_copy.start()
    tell(2)

    for b in range(tokens // 32 - 1):
        norm_rows(b * 32, 32)

    mine = pl.multiple_of((y * 4 + x) * 128, 128)
    start = (z * 2 + c) * tokens

    def mixed_rows(wsum, count):
        pos = start + lax.broadcasted_iota(jnp.int32, (count, 1), 0)
        div = jnp.minimum(pos + 1, window).astype(F32)
        pooled = (wsum / div - ng[0:count, :].astype(F32)).astype(BF16)
        mixed = (mm(pooled, pool_w[...]) * pool_scale[...]).astype(BF16).astype(F32)
        aft[0:count, :] = (res[0:count, pl.ds(mine, 128)].astype(F32) + mixed).astype(BF16)

    band = jnp.where((tj <= ti) & (tj > ti - window), 1.0, 0.0).astype(BF16)
    mixed_rows(mm(band, ng[...]), tokens)
    for e in range(experts):
        pick[e * blk : (e + 1) * blk, :] = jnp.where(code[e : e + 1, :] == place, 1.0, 0.0).astype(BF16)

    rim_copy.wait_recv()
    ri = lax.broadcasted_iota(jnp.int32, (SPAN, SPAN), 0)
    rj = lax.broadcasted_iota(jnp.int32, (SPAN, SPAN), 1)
    bend = jnp.where(rj <= ri, jnp.where(rj > ri - window, 1.0, 0.0), 0.0).astype(BF16)
    over = jnp.where(rj - SPAN > ri - window, 1.0, 0.0) * jnp.where(z * 2 + c > 0, 1.0, 0.0)
    mixed_rows(mm(bend, ng[0:SPAN, :]) + mm(over.astype(BF16), rim[...]), SPAN)

    sent[...] = mm(pick[...], aft[...]).astype(BF16)
    def dispatch(r, dz):
        for rel in range(2):
            zd, cd = (z + (nz - dz) % nz) % nz, (c + rel) % 2
            src = sent.at[pl.ds(pl.multiple_of((zd * 2 + cd) * blk, blk), blk)]
            j = 2 * r + rel
            dst = slots.at[y, x, pl.ds(j * blk, blk)]
            if j:
                pltpu.make_async_remote_copy(
                    src_ref=src, dst_ref=dst, send_sem=dsp_s, recv_sem=dsp_r.at[j // per],
                    device_id={"z": zd, "c": cd}, device_id_type=MESH,
                ).start()
            else:
                pltpu.make_async_copy(src, dst, own_s.at[0]).start()

    for r in range(4):
        dispatch(r, DZ[r])
    told(2)
    tell(4)
    later = sorted(range(4, nz), key=lambda r: abs(DZ[r]))
    for r in later:
        if abs(DZ[r]) <= 4:
            dispatch(r, DZ[r])

    def fill_selection():
        lane = lax.broadcasted_iota(jnp.int32, (tokens, experts * blk), 1).astype(F32)
        for k in range(2):
            sel[k * tokens : (k + 1) * tokens, :] = jnp.where(cols[:, k : k + 1] == lane, 1.0, 0.0).astype(BF16)

    def landed(ref, sem):
        pltpu.make_async_copy(ref, ref, sem).wait()

    def push(src, dst, s, r, to):
        pltpu.make_async_remote_copy(
            src_ref=src, dst_ref=dst, send_sem=s, recv_sem=r, device_id=to, device_id_type=MESH
        ).start()

    DIRS = ((0, 1), (1, 3))
    HALVES = ((0, "x", "y"), (1, "y", "x"))

    def pieces(hl):
        cut = hl * SPLIT // 4
        return ((0, 1, 0, cut), (1, 3, cut, hl - cut))

    def gather_stages(buf, base_of, hl, ss, rs):
        def rows(k, h, off, n):
            return pl.ds(base_of(k) + h * hl + off, n)

        def one(h, d, k, off, n):
            if h == 0:
                return buf.at[y, (x + d) % 4, rows(k, h, off, n)]
            return buf.at[(y + d) % 4, x, rows(k, h, off, n)]

        def line(h, d, k, off, n):
            if h == 0:
                return buf.at[(y + d) % 4, :, rows(k, h, off, n)]
            return buf.at[:, (x + d) % 4, rows(k, h, off, n)]

        def a1(k):
            for d in (1, 3, 2):
                for h, ax, _ in HALVES:
                    push(one(h, 0, k, 0, hl), one(h, 0, k, 0, hl), ss.at[k], rs.at[k, h, 0], along(ax, d))

        def a2(k):
            for h, _, ax in HALVES:
                landed(buf.at[0, pl.ds(0, 3), rows(k, h, 0, hl)], rs.at[k, h, 0])
                for i, d in DIRS:
                    ref = line(h, 0, k, 0, hl)
                    push(ref, ref, ss.at[k], rs.at[k, h, 1 + i], along(ax, d))

        def a3(k):
            for h, _, ax in HALVES:
                for i, d, off, n in pieces(hl):
                    landed(line(h, 4 - d, k, 0, hl), rs.at[k, h, 1 + i])
                    ref = line(h, 4 - d, k, off, n)
                    push(ref, ref, ss.at[k], rs.at[k, h, 3], along(ax, d))

        def a4(k):
            for h, _, _ in HALVES:
                landed(line(h, 2, k, 0, hl), rs.at[k, h, 3])

        def drain(k):
            landed(buf.at[:, :, pl.ds(0, hl * 15 // 8)], ss.at[k])

        return a1, a2, a3, a4, drain

    def base_of(k):
        return k * chunk if isinstance(k, int) else pl.multiple_of(k * chunk, chunk)

    a1, a2, a3, a4, ag_drain = gather_stages(slots, base_of, half, ag_s, ag_r)

    def s0(k):
        if isinstance(k, int):
            landed(slots.at[y, x, pl.ds(0, blk)], own_s.at[0])
            landed(slots.at[y, x, pl.ds(blk, chunk - blk)], dsp_r.at[0])
        else:
            landed(slots.at[y, x, pl.ds(base_of(k), chunk)], dsp_r.at[k])
        a1(k)

    def line(h, d, k, off, n):
        rows = pl.ds(base_of(k) + h * half + off, n)
        if h == 0:
            return part.at[(y + d) % 4, :, rows]
        return part.at[:, (x + d) % 4, rows]

    def one(h, d, k, off, n):
        rows = pl.ds(base_of(k) + h * half + off, n)
        if h == 0:
            return part.at[y, (x + d) % 4, rows]
        return part.at[(y + d) % 4, x, rows]

    SUMS = ((0, "y", "x"), (1, "x", "y"))

    def ffn(k):
        a4(k)

        @pl.when(k == 0)
        def _():
            for copy in loads[1:]:
                copy.wait()

        def norm(b, carry):
            rows = pl.ds(pl.multiple_of(base_of(k) + b * 32, 32), 32)
            total = jnp.zeros((32, 128), F32)
            for t in range(16):
                v = slots[t // 4, t % 4, rows, :].astype(F32)
                total = total + v * v
            inv = lax.rsqrt(jnp.sum(total, axis=1, keepdims=True) / width + EPS)
            put = pl.ds(pl.multiple_of(b * 32, 32), 32)
            for t in range(16):
                v = slots[t // 4, t % 4, rows, :].astype(F32)
                normed[put, t * 128 : (t + 1) * 128] = (
                    v * inv * ffn_gain[:, t * 128 : (t + 1) * 128]
                ).astype(BF16)
            return carry

        lax.fori_loop(0, chunk // 32, norm, 0)
        g = mm(normed[...], gate[...], NT)
        u = mm(normed[...], up[...], NT)
        hidden = (jax.nn.silu(g) * u).astype(BF16)
        rows = pl.ds(base_of(k), chunk)
        for t in range(0, 16, 2):
            p = mm(hidden, down[:, t * 128 : (t + 2) * 128]).astype(BF16)
            part[t // 4, t % 4, rows, :] = p[:, :128]
            part[t // 4, t % 4 + 1, rows, :] = p[:, 128:]
        for h, ax, _ in SUMS:
            for i, d, off, n in pieces(half):
                push(line(h, 2, k, off, n), got1.at[k, h, :, pl.ds(off, n)], rs_s.at[k], rs_r.at[k, h, i], along(ax, d))

    def add(ref, *others):
        total = ref[...].astype(F32)
        for other in others:
            total = total + other[...].astype(F32)
        ref[...] = total.astype(BF16)

    def r2(k):
        for h, ax, _ in SUMS:
            for i, d, off, n in pieces(half):
                landed(got1.at[k, h, :, pl.ds(off, n)], rs_r.at[k, h, i])
                add(line(h, d, k, off, n), got1.at[k, h, :, pl.ds(off, n)])
                push(line(h, d, k, 0, half), got2.at[k, h, i], rs_s.at[k], rs_r.at[k, h, 2], along(ax, d))

    def r3(k):
        for h, _, ax in SUMS:
            landed(got2.at[k, h], rs_r.at[k, h, 2])
            add(line(h, 0, k, 0, half), got2.at[k, h, 0], got2.at[k, h, 1])
            for d in (2, 1, 3):
                push(one(h, d, k, 0, half), got3.at[k, h, d - 1], rs_s.at[k], rs_r.at[k, h, 3], along(ax, d))

    home = pl.ds(pl.multiple_of((z * 2 + c) * blk, blk), blk)

    def back(k):
        for h, _, _ in SUMS:
            landed(got3.at[k, h], rs_r.at[k, h, 3])
            total = one(h, 0, k, 0, half)[...].astype(F32)
            for d in (1, 2, 3):
                total = total + got3[k, h, d - 1].astype(F32)
            summed[pl.ds(base_of(k) + h * half, half), :] = total.astype(BF16)
        for kk in range(NC):

            @pl.when(k == kk)
            def _(kk=kk):
                for i in range(per):
                    j = kk * per + i
                    src = summed.at[pl.ds(j * blk, blk)]
                    to = {"z": (z + (DZ[j // 2] + nz) % nz) % nz, "c": (c + j % 2) % 2}
                    if j:
                        push(src, ret.at[home], ret_s, ret_r, to)
                    else:
                        pltpu.make_async_copy(src, ret.at[home], own_s.at[1]).start()

    def rs_drain(k):
        landed(part.at[:, :, pl.ds(0, chunk * 15 // 16)], rs_s.at[k])

    stages = (s0, a2, a3, ffn, r2, r3, back)

    def step(tau, carry):
        for s in ORDER:
            k = tau - s

            @pl.when((k >= 0) & (k < NC))
            def _(s=s, k=k):
                stages[s](k)

        return carry

    s0(0)
    told(4)
    for r in later:
        if abs(DZ[r]) > 4:
            dispatch(r, DZ[r])
    fill_selection()
    lax.fori_loop(1, NC + len(stages) - 1, step, 0)

    landed(ret.at[pl.ds(0, blk)], own_s.at[1])
    landed(ret.at[pl.ds(blk, (experts - 1) * blk)], ret_r)
    picked = mm(sel[...], ret[...])
    mix = cols[:, 2:3] * picked[:tokens] + cols[:, 3:4] * picked[tokens:]
    out[y, x, :, :] = (aft[...].astype(F32) + mix).astype(BF16)
    oc = tokens // NO
    *over_out, og_drain = gather_stages(out, lambda k: k * oc, oc // 2, og_s, og_r)
    for tau in range(NO + 3):
        for s, stage in enumerate(over_out):
            if 0 <= tau - s < NO:
                stage(tau - s)
    rim_copy.wait_send()
    landed(sent.at[pl.ds(0, (experts - 1) * blk)], dsp_s)
    landed(summed.at[pl.ds(0, (experts - 1) * blk)], ret_s)

    def drains(k, carry):
        ag_drain(k)
        rs_drain(k)
        return carry

    lax.fori_loop(0, NC, drains, 0)
    for k in range(NO):
        og_drain(k)


def lay_out(src, dst, sem):
    copies = [
        pltpu.make_async_copy(src.at[t // 4, t % 4], dst.at[:, pl.ds(t * 128, 128)], sem.at[t])
        for t in range(16)
    ]
    for copy in copies:
        copy.start()
    for copy in copies:
        copy.wait()


def shards(res, mix_gain, pool_w, pool_scale, ffn_gain, ids, wts, gate, up, down):
    nz = lax.axis_size("z")
    tokens, width = res.shape
    ff = gate.shape[2]
    experts = nz * 2
    blk = tokens * 2 // 16
    total = experts * blk
    chunk = total // NC
    vmem, hbm = pl.BlockSpec(memory_space=pltpu.VMEM), pl.BlockSpec(memory_space=pl.ANY)
    dma, V = pltpu.SemaphoreType.DMA, pltpu.VMEM
    out = pl.pallas_call(
        functools.partial(kernel, nz),
        name="layer",
        out_shape=pltpu.VMEM((4, 4, tokens, 128), BF16),
        in_specs=[hbm, vmem, vmem, vmem, vmem, vmem, vmem, hbm, hbm, hbm],
        out_specs=vmem,
        scratch_shapes=[
            V((tokens, width), BF16),
            V((ff, width), BF16),
            V((ff, width), BF16),
            V((ff, width), BF16),
            V((tokens, width // GROUPS), BF16),
            V((SPAN, width // GROUPS), BF16),
            V((tokens, 128), BF16),
            V((total, tokens), BF16),
            V((experts, tokens), F32),
            V((2 * tokens, total), BF16),
            V((tokens, 8), F32),
            V((total, 128), BF16),
            V((4, 4, total, 128), BF16),
            V((4, 4, total, 128), BF16),
            V((NC, 2, 4, chunk // 2, 128), BF16),
            V((NC, 2, 2, 4, chunk // 2, 128), BF16),
            V((NC, 2, 3, chunk // 2, 128), BF16),
            V((total, 128), BF16),
            V((total, 128), BF16),
            V((chunk, width), BF16),
            dma((4,)),
            dma, dma, dma, dma((NC,)), dma, dma, dma((2,)),
            dma((NC,)), dma((NC, 2, 4)), dma((NC,)), dma((NC, 2, 4)),
            dma((NO,)), dma((NO, 2, 4)),
            pltpu.SemaphoreType.REGULAR((2,)),
        ],
        compiler_params=pltpu.CompilerParams(
            collective_id=0, has_side_effects=True, vmem_limit_bytes=58 * 1024 * 1024
        ),
    )(
        res, mix_gain.reshape(1, -1), pool_w, pool_scale.reshape(1, -1), ffn_gain.reshape(1, -1),
        ids.T, wts.T, gate[0].T, up[0].T, down[0],
    )
    return pl.pallas_call(
        lay_out,
        name="lay_out",
        out_shape=jax.ShapeDtypeStruct((tokens, width), BF16),
        in_specs=[vmem],
        out_specs=hbm,
        scratch_shapes=[dma((16,))],
        compiler_params=pltpu.CompilerParams(vmem_limit_bytes=4 * 1024 * 1024),
    )(out)


def solution(mesh):
    torus = Mesh(mesh.devices.reshape(mesh.shape["sp"] // 2, 2, 4, 4), AXES)
    sp, tp = ("z", "c"), ("y", "x")
    return jax.shard_map(
        shards,
        mesh=torus,
        in_specs=(
            P(sp, None),
            P(),
            P(None, tp),
            P(tp),
            P(),
            P(sp, None),
            P(sp, None),
            P(sp, None, tp),
            P(sp, None, tp),
            P(sp, tp, None),
        ),
        out_specs=P(sp, None),
        check_vma=False,
    )
```

```python
import functools

import jax
import jax.numpy as jnp
from jax import lax
from jax.experimental import pallas as pl
from jax.experimental.pallas import tpu as pltpu
from jax.sharding import Mesh
from jax.sharding import PartitionSpec as P

MESH = pl.DeviceIdType.MESH
AXES = ("z", "c", "y", "x")
EPS = 1e-06
GROUPS = 4
SPAN = 16
NC = 4
ORDER = (2, 1, 0, 3, 4, 5, 6)
NO = 2
DZ = (0, 1, -1, 2, -2, 3, -3, 4, -6, 7, -7, 8, -4, 5, -5, 6)
SPLIT = 2
F32, BF16 = jnp.float32, jnp.bfloat16
NN = (((1,), (0,)), ((), ()))
NT = (((1,), (1,)), ((), ()))


def mm(a, b, dims=NN):
    return lax.dot_general(a, b, dims, preferred_element_type=F32)


def kernel(
    nz,
    res_any, mix_any, pw_any, ps_any, ffn_any, ids_any, wts_any, gate_any, up_any, down_any,
    out,
    mix_gain, pool_w, pool_scale, ffn_gain, ids, wts, res, gate, up, down, ng, rim, aft, pick, code, sel, cols,
    sent, slots, part, got1, got2, got3, summed, ret, normed,
    lsem, rim_s, rim_r, dsp_s, dsp_r, ret_s, ret_r, own_s, ag_s, ag_r, rs_s, rs_r, og_s, og_r, tok,
):
    tokens, width = res.shape
    group = width // GROUPS
    experts = nz * 2
    blk = tokens * 2 // 16
    chunk = experts * blk // NC
    half, quart = chunk // 2, chunk // 4
    per = experts // NC
    z, c, y, x = (lax.axis_index(a) for a in AXES)

    def along(axis, d):
        return {axis: ({"x": x, "y": y}[axis] + d) % 4}

    loads = [
        pltpu.make_async_copy(s, d, lsem.at[i])
        for i, (s, d) in enumerate(
            (
                (ids_any, ids), (wts_any, wts), (res_any, res), (mix_any, mix_gain), (pw_any, pool_w),
                (ps_any, pool_scale), (ffn_any, ffn_gain), (gate_any, gate), (up_any, up), (down_any, down),
            )
        )
    ]
    for copy in loads[:6]:
        copy.start()

    barrier = pltpu.get_barrier_semaphore()
    for r in (0, 1, 2, nz - 2, nz - 1):
        for rel in range(2):
            if r or rel:
                pl.semaphore_signal(
                    barrier, 1, device_id={"z": (z + r) % nz, "c": (c + rel) % 2}, device_id_type=MESH
                )
    for axis in ("x", "y"):
        for d in (1, 2, 3):
            pl.semaphore_signal(barrier, 1, device_id=along(axis, d), device_id_type=MESH)

    def tell(r):
        for d in (r, nz - r):
            pl.semaphore_signal(tok.at[r // 4], 1, device_id={"z": (z + d) % nz}, device_id_type=MESH)

    def told(r):
        pl.semaphore_wait(tok.at[r // 4], 2)

    window = lax.shift_left(jnp.int32(1), y + 1)
    first = pl.multiple_of(y * group, group)
    def norm_rows(at, n):
        rows = pl.ds(at, n)
        gain = mix_gain[:, pl.ds(first, group)]
        v = res[rows, :].astype(F32)
        inv = lax.rsqrt(jnp.sum(v * v, axis=1, keepdims=True) / width + EPS)
        ng[rows, :] = (res[rows, pl.ds(first, group)].astype(F32) * inv * gain).astype(BF16)

    for copy in loads[:2]:
        copy.wait()
    eid = lax.broadcasted_iota(jnp.int32, (experts, tokens), 0)
    m0, m1 = ids[0:1, :] == eid, ids[1:2, :] == eid
    ti = lax.broadcasted_iota(jnp.int32, (tokens, tokens), 0)
    tj = lax.broadcasted_iota(jnp.int32, (tokens, tokens), 1)
    named = jnp.where(m0 | m1, 1.0, 0.0)
    before = mm(named.astype(BF16), jnp.where(ti < tj, 1.0, 0.0).astype(BF16))
    code[...] = jnp.where(m0 | m1, before, -1.0)
    target = eid.astype(F32) * blk + before
    t0 = jnp.sum(jnp.where(m0, target, 0.0), axis=0, keepdims=True)
    t1 = jnp.sum(jnp.where(m1, target, 0.0), axis=0, keepdims=True)
    tall = jnp.concatenate([t0, t1, wts[0:1, :], wts[1:2, :], jnp.zeros((4, tokens), F32)], axis=0)
    cols[...] = jnp.transpose(tall)
    place = lax.broadcasted_iota(jnp.int32, (blk, tokens), 0).astype(F32)

    for copy in loads[2:6]:
        copy.wait()
    for copy in loads[6:]:
        copy.start()
    norm_rows(tokens - 32, 32)
    pl.semaphore_wait(barrier, 15)
    nxt = {"z": (z + c) % nz, "c": (c + 1) % 2}
    rim_copy = pltpu.make_async_remote_copy(
        src_ref=ng.at[pl.ds(tokens - SPAN, SPAN)], dst_ref=rim, send_sem=rim_s, recv_sem=rim_r,
        device_id=nxt, device_id_type=MESH,
    )
    rim_copy.start()
    tell(2)

    for b in range(tokens // 32 - 1):
        norm_rows(b * 32, 32)

    mine = pl.multiple_of((y * 4 + x) * 128, 128)
    start = (z * 2 + c) * tokens

    def mixed_rows(wsum, count):
        pos = start + lax.broadcasted_iota(jnp.int32, (count, 1), 0)
        div = jnp.minimum(pos + 1, window).astype(F32)
        pooled = (wsum / div - ng[0:count, :].astype(F32)).astype(BF16)
        mixed = (mm(pooled, pool_w[...]) * pool_scale[...]).astype(BF16).astype(F32)
        aft[0:count, :] = (res[0:count, pl.ds(mine, 128)].astype(F32) + mixed).astype(BF16)

    band = jnp.where((tj <= ti) & (tj > ti - window), 1.0, 0.0).astype(BF16)
    mixed_rows(mm(band, ng[...]), tokens)
    for e in range(experts):
        pick[e * blk : (e + 1) * blk, :] = jnp.where(code[e : e + 1, :] == place, 1.0, 0.0).astype(BF16)

    rim_copy.wait_recv()
    ri = lax.broadcasted_iota(jnp.int32, (SPAN, SPAN), 0)
    rj = lax.broadcasted_iota(jnp.int32, (SPAN, SPAN), 1)
    bend = jnp.where(rj <= ri, jnp.where(rj > ri - window, 1.0, 0.0), 0.0).astype(BF16)
    over = jnp.where(rj - SPAN > ri - window, 1.0, 0.0) * jnp.where(z * 2 + c > 0, 1.0, 0.0)
    mixed_rows(mm(bend, ng[0:SPAN, :]) + mm(over.astype(BF16), rim[...]), SPAN)

    sent[...] = mm(pick[...], aft[...]).astype(BF16)
    def dispatch(r, dz):
        for rel in range(2):
            zd, cd = (z + (nz - dz) % nz) % nz, (c + rel) % 2
            src = sent.at[pl.ds(pl.multiple_of((zd * 2 + cd) * blk, blk), blk)]
            j = 2 * r + rel
            dst = slots.at[y, x, pl.ds(j * blk, blk)]
            if j:
                pltpu.make_async_remote_copy(
                    src_ref=src, dst_ref=dst, send_sem=dsp_s, recv_sem=dsp_r.at[j // per],
                    device_id={"z": zd, "c": cd}, device_id_type=MESH,
                ).start()
            else:
                pltpu.make_async_copy(src, dst, own_s.at[0]).start()

    for r in range(4):
        dispatch(r, DZ[r])
    told(2)
    tell(4)
    later = sorted(range(4, nz), key=lambda r: abs(DZ[r]))
    for r in later:
        if abs(DZ[r]) <= 4:
            dispatch(r, DZ[r])

    def fill_selection():
        lane = lax.broadcasted_iota(jnp.int32, (tokens, experts * blk), 1).astype(F32)
        for k in range(2):
            sel[k * tokens : (k + 1) * tokens, :] = jnp.where(cols[:, k : k + 1] == lane, 1.0, 0.0).astype(BF16)

    def landed(ref, sem):
        pltpu.make_async_copy(ref, ref, sem).wait()

    def push(src, dst, s, r, to):
        pltpu.make_async_remote_copy(
            src_ref=src, dst_ref=dst, send_sem=s, recv_sem=r, device_id=to, device_id_type=MESH
        ).start()

    DIRS = ((0, 1), (1, 3))
    HALVES = ((0, "x", "y"), (1, "y", "x"))

    def pieces(hl):
        cut = hl * SPLIT // 4
        return ((0, 1, 0, cut), (1, 3, cut, hl - cut))

    def gather_stages(buf, base_of, hl, ss, rs, direct=False):
        def rows(k, h, off, n):
            return pl.ds(base_of(k) + h * hl + off, n)

        def one(h, d, k, off, n):
            if h == 0:
                return buf.at[y, (x + d) % 4, rows(k, h, off, n)]
            return buf.at[(y + d) % 4, x, rows(k, h, off, n)]

        def line(h, d, k, off, n):
            if h == 0:
                return buf.at[(y + d) % 4, :, rows(k, h, off, n)]
            return buf.at[:, (x + d) % 4, rows(k, h, off, n)]

        def a1(k):
            for d in (1, 3, 2):
                for h, ax, _ in HALVES:
                    push(one(h, 0, k, 0, hl), one(h, 0, k, 0, hl), ss.at[k], rs.at[k, h, 0], along(ax, d))

        def a2(k):
            for h, _, ax in HALVES:
                landed(buf.at[0, pl.ds(0, 3), rows(k, h, 0, hl)], rs.at[k, h, 0])
                for i, d in DIRS + ((2, 2),) * direct:
                    ref = line(h, 0, k, 0, hl)
                    push(ref, ref, ss.at[k], rs.at[k, h, 1 + i], along(ax, d))

        def a3(k):
            for h, _, ax in HALVES:
                for i, d, off, n in pieces(hl):
                    landed(line(h, 4 - d, k, 0, hl), rs.at[k, h, 1 + i])
                    ref = line(h, 4 - d, k, off, n)
                    push(ref, ref, ss.at[k], rs.at[k, h, 3], along(ax, d))

        def a4(k):
            for h, _, _ in HALVES:
                landed(line(h, 2, k, 0, hl), rs.at[k, h, 3])

        def drain(k):
            landed(buf.at[:, :, pl.ds(0, hl * 15 // 8)], ss.at[k])

        def a34(k):
            for h in (0, 1):
                for i, d in DIRS + ((2, 2),):
                    landed(line(h, 4 - d, k, 0, hl), rs.at[k, h, 1 + i])

        return (a1, a2, a34, drain) if direct else (a1, a2, a3, a4, drain)

    def base_of(k):
        return k * chunk if isinstance(k, int) else pl.multiple_of(k * chunk, chunk)

    a1, a2, a3, a4, ag_drain = gather_stages(slots, base_of, half, ag_s, ag_r)

    def s0(k):
        if isinstance(k, int):
            landed(slots.at[y, x, pl.ds(0, blk)], own_s.at[0])
            landed(slots.at[y, x, pl.ds(blk, chunk - blk)], dsp_r.at[0])
        else:
            landed(slots.at[y, x, pl.ds(base_of(k), chunk)], dsp_r.at[k])
        a1(k)

    def line(h, d, k, off, n):
        rows = pl.ds(base_of(k) + h * half + off, n)
        if h == 0:
            return part.at[(y + d) % 4, :, rows]
        return part.at[:, (x + d) % 4, rows]

    def one(h, d, k, off, n):
        rows = pl.ds(base_of(k) + h * half + off, n)
        if h == 0:
            return part.at[y, (x + d) % 4, rows]
        return part.at[(y + d) % 4, x, rows]

    SUMS = ((0, "y", "x"), (1, "x", "y"))

    def ffn(k):
        a4(k)

        @pl.when(k == 0)
        def _():
            for copy in loads[6:]:
                copy.wait()

        def norm(b, carry):
            rows = pl.ds(pl.multiple_of(base_of(k) + b * 32, 32), 32)
            total = jnp.zeros((32, 128), F32)
            for t in range(16):
                v = slots[t // 4, t % 4, rows, :].astype(F32)
                total = total + v * v
            inv = lax.rsqrt(jnp.sum(total, axis=1, keepdims=True) / width + EPS)
            put = pl.ds(pl.multiple_of(b * 32, 32), 32)
            for t in range(16):
                v = slots[t // 4, t % 4, rows, :].astype(F32)
                normed[put, t * 128 : (t + 1) * 128] = (
                    v * inv * ffn_gain[:, t * 128 : (t + 1) * 128]
                ).astype(BF16)
            return carry

        lax.fori_loop(0, chunk // 32, norm, 0)
        g = mm(normed[...], gate[...], NT)
        u = mm(normed[...], up[...], NT)
        hidden = (jax.nn.silu(g) * u).astype(BF16)
        rows = pl.ds(base_of(k), chunk)
        for t in range(0, 16, 2):
            p = mm(hidden, down[:, t * 128 : (t + 2) * 128]).astype(BF16)
            part[t // 4, t % 4, rows, :] = p[:, :128]
            part[t // 4, t % 4 + 1, rows, :] = p[:, 128:]
        for h, ax, _ in SUMS:
            for i, d, off, n in pieces(half):
                push(line(h, 2, k, off, n), got1.at[k, h, :, pl.ds(off, n)], rs_s.at[k], rs_r.at[k, h, i], along(ax, d))

    def add(ref, *others):
        total = ref[...].astype(F32)
        for other in others:
            total = total + other[...].astype(F32)
        ref[...] = total.astype(BF16)

    def r2(k):
        for h, ax, _ in SUMS:
            for i, d, off, n in pieces(half):
                landed(got1.at[k, h, :, pl.ds(off, n)], rs_r.at[k, h, i])
                add(line(h, d, k, off, n), got1.at[k, h, :, pl.ds(off, n)])
                push(line(h, d, k, 0, half), got2.at[k, h, i], rs_s.at[k], rs_r.at[k, h, 2], along(ax, d))

    def r3(k):
        for h, _, ax in SUMS:
            landed(got2.at[k, h], rs_r.at[k, h, 2])
            add(line(h, 0, k, 0, half), got2.at[k, h, 0], got2.at[k, h, 1])
            for d in (2, 1, 3):
                push(one(h, d, k, 0, half), got3.at[k, h, d - 1], rs_s.at[k], rs_r.at[k, h, 3], along(ax, d))

    home = pl.ds(pl.multiple_of((z * 2 + c) * blk, blk), blk)

    def back(k):
        for h, _, _ in SUMS:
            landed(got3.at[k, h], rs_r.at[k, h, 3])
            total = one(h, 0, k, 0, half)[...].astype(F32)
            for d in (1, 2, 3):
                total = total + got3[k, h, d - 1].astype(F32)
            summed[pl.ds(base_of(k) + h * half, half), :] = total.astype(BF16)
        for kk in range(NC):

            @pl.when(k == kk)
            def _(kk=kk):
                for i in reversed(range(per)):
                    j = kk * per + i
                    src = summed.at[pl.ds(j * blk, blk)]
                    to = {"z": (z + (DZ[j // 2] + nz) % nz) % nz, "c": (c + j % 2) % 2}
                    if j:
                        push(src, ret.at[home], ret_s, ret_r, to)
                    else:
                        pltpu.make_async_copy(src, ret.at[home], own_s.at[1]).start()

    def rs_drain(k):
        landed(part.at[:, :, pl.ds(0, chunk * 15 // 16)], rs_s.at[k])

    stages = (s0, a2, a3, ffn, r2, r3, back)

    def step(tau, carry):
        for s in ORDER:
            k = tau - s

            @pl.when((k >= 0) & (k < NC))
            def _(s=s, k=k):
                stages[s](k)

        return carry

    s0(0)
    told(4)
    for r in sorted(later, key=lambda r: (r // 4, -abs(DZ[r]))):
        if abs(DZ[r]) > 4:
            dispatch(r, DZ[r])
    fill_selection()
    lax.fori_loop(1, NC + len(stages) - 1, step, 0)

    landed(ret.at[pl.ds(0, blk)], own_s.at[1])
    landed(ret.at[pl.ds(blk, (experts - 1) * blk)], ret_r)
    picked = mm(sel[...], ret[...])
    mix = cols[:, 2:3] * picked[:tokens] + cols[:, 3:4] * picked[tokens:]
    out[y, x, :, :] = (aft[...].astype(F32) + mix).astype(BF16)
    oc = tokens // NO
    *over_out, og_drain = gather_stages(out, lambda k: k * oc, oc // 2, og_s, og_r, True)
    for tau in range(NO + len(over_out) - 1):
        for s, stage in enumerate(over_out):
            if 0 <= tau - s < NO:
                stage(tau - s)
    rim_copy.wait_send()
    landed(sent.at[pl.ds(0, (experts - 1) * blk)], dsp_s)
    landed(summed.at[pl.ds(0, (experts - 1) * blk)], ret_s)

    def drains(k, carry):
        ag_drain(k)
        rs_drain(k)
        return carry

    lax.fori_loop(0, NC, drains, 0)
    for k in range(NO):
        og_drain(k)


def lay_out(src, dst, sem):
    copies = [
        pltpu.make_async_copy(src.at[t // 4, t % 4], dst.at[:, pl.ds(t * 128, 128)], sem.at[t])
        for t in range(16)
    ]
    for copy in copies:
        copy.start()
    for copy in copies:
        copy.wait()


def shards(res, mix_gain, pool_w, pool_scale, ffn_gain, ids, wts, gate, up, down):
    nz = lax.axis_size("z")
    tokens, width = res.shape
    ff = gate.shape[2]
    experts = nz * 2
    blk = tokens * 2 // 16
    total = experts * blk
    chunk = total // NC
    vmem, hbm = pl.BlockSpec(memory_space=pltpu.VMEM), pl.BlockSpec(memory_space=pl.ANY)
    dma, V = pltpu.SemaphoreType.DMA, pltpu.VMEM
    out = pl.pallas_call(
        functools.partial(kernel, nz),
        name="layer",
        out_shape=pltpu.VMEM((4, 4, tokens, 128), BF16),
        in_specs=[hbm] * 10,
        out_specs=vmem,
        scratch_shapes=[
            V((1, width), F32),
            V(pool_w.shape, BF16),
            V((1, 128), F32),
            V((1, width), F32),
            V((2, tokens), jnp.int32),
            V((2, tokens), F32),
            V((tokens, width), BF16),
            V((ff, width), BF16),
            V((ff, width), BF16),
            V((ff, width), BF16),
            V((tokens, width // GROUPS), BF16),
            V((SPAN, width // GROUPS), BF16),
            V((tokens, 128), BF16),
            V((total, tokens), BF16),
            V((experts, tokens), F32),
            V((2 * tokens, total), BF16),
            V((tokens, 8), F32),
            V((total, 128), BF16),
            V((4, 4, total, 128), BF16),
            V((4, 4, total, 128), BF16),
            V((NC, 2, 4, chunk // 2, 128), BF16),
            V((NC, 2, 2, 4, chunk // 2, 128), BF16),
            V((NC, 2, 3, chunk // 2, 128), BF16),
            V((total, 128), BF16),
            V((total, 128), BF16),
            V((chunk, width), BF16),
            dma((10,)),
            dma, dma, dma, dma((NC,)), dma, dma, dma((2,)),
            dma((NC,)), dma((NC, 2, 4)), dma((NC,)), dma((NC, 2, 4)),
            dma((NO,)), dma((NO, 2, 4)),
            pltpu.SemaphoreType.REGULAR((2,)),
        ],
        compiler_params=pltpu.CompilerParams(
            collective_id=0, has_side_effects=True, vmem_limit_bytes=58 * 1024 * 1024
        ),
    )(
        res, mix_gain.reshape(1, -1), pool_w, pool_scale.reshape(1, -1), ffn_gain.reshape(1, -1),
        ids.T, wts.T, gate[0].T, up[0].T, down[0],
    )
    return pl.pallas_call(
        lay_out,
        name="lay_out",
        out_shape=jax.ShapeDtypeStruct((tokens, width), BF16),
        in_specs=[vmem],
        out_specs=hbm,
        scratch_shapes=[dma((16,))],
        compiler_params=pltpu.CompilerParams(vmem_limit_bytes=4 * 1024 * 1024),
    )(out)


def solution(mesh):
    torus = Mesh(mesh.devices.reshape(mesh.shape["sp"] // 2, 2, 4, 4), AXES)
    sp, tp = ("z", "c"), ("y", "x")
    return jax.shard_map(
        shards,
        mesh=torus,
        in_specs=(
            P(sp, None),
            P(),
            P(None, tp),
            P(tp),
            P(),
            P(sp, None),
            P(sp, None),
            P(sp, None, tp),
            P(sp, None, tp),
            P(sp, tp, None),
        ),
        out_specs=P(sp, None),
        check_vma=False,
    )
```

```python
import functools

import jax
import jax.numpy as jnp
from jax import lax
from jax.experimental import pallas as pl
from jax.experimental.pallas import tpu as pltpu
from jax.sharding import Mesh
from jax.sharding import PartitionSpec as P

MESH = pl.DeviceIdType.MESH
AXES = ("z", "c", "y", "x")
EPS = 1e-06
GROUPS = 4
SPAN = 16
NC = 4
ORDER = (2, 1, 0, 3, 4, 5, 6)
NO = 2
DZ = (0, 1, -1, 2, -2, 3, -3, 4, -4, 5, -5, 6, -6, 7, -7, 8)
SPLIT = 2
F32, BF16 = jnp.float32, jnp.bfloat16
NN = (((1,), (0,)), ((), ()))
NT = (((1,), (1,)), ((), ()))


def mm(a, b, dims=NN):
    return lax.dot_general(a, b, dims, preferred_element_type=F32)


def kernel(
    nz,
    res_any, mix_any, pw_any, ps_any, ffn_any, ids_any, wts_any, gate_any, up_any, down_any,
    out,
    mix_gain, pool_w, pool_scale, ffn_gain, ids, wts, res, gate, up, down, ng, rim, aft, pick, code, sel, cols,
    sent, slots, part, got1, got2, got3, summed, ret, normed,
    lsem, rim_s, rim_r, dsp_s, dsp_r, ret_s, ret_r, own_s, ag_s, ag_r, rs_s, rs_r, og_s, og_r, tok,
):
    tokens, width = res.shape
    group = width // GROUPS
    experts = nz * 2
    blk = tokens * 2 // 16
    chunk = experts * blk // NC
    half, quart = chunk // 2, chunk // 4
    per = experts // NC
    z, c, y, x = (lax.axis_index(a) for a in AXES)

    def along(axis, d):
        return {axis: ({"x": x, "y": y}[axis] + d) % 4}

    loads = [
        pltpu.make_async_copy(s, d, lsem.at[i])
        for i, (s, d) in enumerate(
            (
                (ids_any, ids), (wts_any, wts), (res_any, res), (mix_any, mix_gain), (pw_any, pool_w),
                (ps_any, pool_scale), (ffn_any, ffn_gain), (gate_any, gate), (up_any, up), (down_any, down),
            )
        )
    ]
    for copy in loads[:6]:
        copy.start()

    barrier = pltpu.get_barrier_semaphore()
    for r in (0, 1, 2, nz - 2, nz - 1):
        for rel in range(2):
            if r or rel:
                pl.semaphore_signal(
                    barrier, 1, device_id={"z": (z + r) % nz, "c": (c + rel) % 2}, device_id_type=MESH
                )
    for axis in ("x", "y"):
        for d in (1, 2, 3):
            pl.semaphore_signal(barrier, 1, device_id=along(axis, d), device_id_type=MESH)

    def tell(r):
        for d in (r, nz - r):
            pl.semaphore_signal(tok.at[r // 4], 1, device_id={"z": (z + d) % nz}, device_id_type=MESH)

    def told(r):
        pl.semaphore_wait(tok.at[r // 4], 2)

    window = lax.shift_left(jnp.int32(1), y + 1)
    first = pl.multiple_of(y * group, group)
    def norm_rows(at, n):
        rows = pl.ds(at, n)
        gain = mix_gain[:, pl.ds(first, group)]
        v = res[rows, :].astype(F32)
        inv = lax.rsqrt(jnp.sum(v * v, axis=1, keepdims=True) / width + EPS)
        ng[rows, :] = (res[rows, pl.ds(first, group)].astype(F32) * inv * gain).astype(BF16)

    for copy in loads[:2]:
        copy.wait()
    eid = lax.broadcasted_iota(jnp.int32, (experts, tokens), 0)
    m0, m1 = ids[0:1, :] == eid, ids[1:2, :] == eid
    ti = lax.broadcasted_iota(jnp.int32, (tokens, tokens), 0)
    tj = lax.broadcasted_iota(jnp.int32, (tokens, tokens), 1)
    named = jnp.where(m0 | m1, 1.0, 0.0)
    before = mm(named.astype(BF16), jnp.where(ti < tj, 1.0, 0.0).astype(BF16))
    code[...] = jnp.where(m0 | m1, before, -1.0)
    target = eid.astype(F32) * blk + before
    t0 = jnp.sum(jnp.where(m0, target, 0.0), axis=0, keepdims=True)
    t1 = jnp.sum(jnp.where(m1, target, 0.0), axis=0, keepdims=True)
    tall = jnp.concatenate([t0, t1, wts[0:1, :], wts[1:2, :], jnp.zeros((4, tokens), F32)], axis=0)
    cols[...] = jnp.transpose(tall)
    place = lax.broadcasted_iota(jnp.int32, (blk, tokens), 0).astype(F32)

    for copy in loads[2:6]:
        copy.wait()
    for copy in loads[6:]:
        copy.start()
    norm_rows(tokens - 32, 32)
    pl.semaphore_wait(barrier, 15)
    nxt = {"z": (z + c) % nz, "c": (c + 1) % 2}
    rim_copy = pltpu.make_async_remote_copy(
        src_ref=ng.at[pl.ds(tokens - SPAN, SPAN)], dst_ref=rim, send_sem=rim_s, recv_sem=rim_r,
        device_id=nxt, device_id_type=MESH,
    )
    rim_copy.start()
    tell(2)

    for b in range(tokens // 32 - 1):
        norm_rows(b * 32, 32)

    mine = pl.multiple_of((y * 4 + x) * 128, 128)
    start = (z * 2 + c) * tokens

    def mixed_rows(wsum, count):
        pos = start + lax.broadcasted_iota(jnp.int32, (count, 1), 0)
        div = jnp.minimum(pos + 1, window).astype(F32)
        pooled = (wsum / div - ng[0:count, :].astype(F32)).astype(BF16)
        mixed = (mm(pooled, pool_w[...]) * pool_scale[...]).astype(BF16).astype(F32)
        aft[0:count, :] = (res[0:count, pl.ds(mine, 128)].astype(F32) + mixed).astype(BF16)

    band = jnp.where((tj <= ti) & (tj > ti - window), 1.0, 0.0).astype(BF16)
    mixed_rows(mm(band, ng[...]), tokens)
    for e in range(experts):
        pick[e * blk : (e + 1) * blk, :] = jnp.where(code[e : e + 1, :] == place, 1.0, 0.0).astype(BF16)

    rim_copy.wait_recv()
    ri = lax.broadcasted_iota(jnp.int32, (SPAN, SPAN), 0)
    rj = lax.broadcasted_iota(jnp.int32, (SPAN, SPAN), 1)
    bend = jnp.where(rj <= ri, jnp.where(rj > ri - window, 1.0, 0.0), 0.0).astype(BF16)
    over = jnp.where(rj - SPAN > ri - window, 1.0, 0.0) * jnp.where(z * 2 + c > 0, 1.0, 0.0)
    mixed_rows(mm(bend, ng[0:SPAN, :]) + mm(over.astype(BF16), rim[...]), SPAN)

    sent[...] = mm(pick[...], aft[...]).astype(BF16)
    def dispatch(r, dz):
        for rel in range(2):
            zd, cd = (z + (nz - dz) % nz) % nz, (c + rel) % 2
            src = sent.at[pl.ds(pl.multiple_of((zd * 2 + cd) * blk, blk), blk)]
            j = 2 * r + rel
            dst = slots.at[y, x, pl.ds(j * blk, blk)]
            if j:
                pltpu.make_async_remote_copy(
                    src_ref=src, dst_ref=dst, send_sem=dsp_s, recv_sem=dsp_r.at[j // per],
                    device_id={"z": zd, "c": cd}, device_id_type=MESH,
                ).start()
            else:
                pltpu.make_async_copy(src, dst, own_s.at[0]).start()

    for r in range(4):
        dispatch(r, DZ[r])
    told(2)
    tell(4)
    later = sorted(range(4, nz), key=lambda r: abs(DZ[r]))
    for r in later:
        if abs(DZ[r]) <= 4:
            dispatch(r, DZ[r])

    def fill_selection():
        lane = lax.broadcasted_iota(jnp.int32, (tokens, experts * blk), 1).astype(F32)
        for k in range(2):
            sel[k * tokens : (k + 1) * tokens, :] = jnp.where(cols[:, k : k + 1] == lane, 1.0, 0.0).astype(BF16)

    def landed(ref, sem):
        pltpu.make_async_copy(ref, ref, sem).wait()

    def push(src, dst, s, r, to):
        pltpu.make_async_remote_copy(
            src_ref=src, dst_ref=dst, send_sem=s, recv_sem=r, device_id=to, device_id_type=MESH
        ).start()

    DIRS = ((0, 1), (1, 3))
    HALVES = ((0, "x", "y"), (1, "y", "x"))

    def pieces(hl):
        cut = hl * SPLIT // 4
        return ((0, 1, 0, cut), (1, 3, cut, hl - cut))

    def gather_stages(buf, base_of, hl, ss, rs, direct=False):
        def rows(k, h, off, n):
            return pl.ds(base_of(k) + h * hl + off, n)

        def one(h, d, k, off, n):
            if h == 0:
                return buf.at[y, (x + d) % 4, rows(k, h, off, n)]
            return buf.at[(y + d) % 4, x, rows(k, h, off, n)]

        def line(h, d, k, off, n):
            if h == 0:
                return buf.at[(y + d) % 4, :, rows(k, h, off, n)]
            return buf.at[:, (x + d) % 4, rows(k, h, off, n)]

        def a1(k):
            for d in (2, 1, 3):
                for h, ax, _ in HALVES:
                    push(one(h, 0, k, 0, hl), one(h, 0, k, 0, hl), ss.at[k], rs.at[k, h, 0], along(ax, d))

        def a2(k):
            for h, _, ax in HALVES:
                landed(buf.at[0, pl.ds(0, 3), rows(k, h, 0, hl)], rs.at[k, h, 0])
                for i, d in ((2, 2),) * direct + DIRS:
                    ref = line(h, 0, k, 0, hl)
                    push(ref, ref, ss.at[k], rs.at[k, h, 1 + i], along(ax, d))

        def a3(k):
            for h, _, ax in HALVES:
                for i, d, off, n in pieces(hl):
                    landed(line(h, 4 - d, k, 0, hl), rs.at[k, h, 1 + i])
                    ref = line(h, 4 - d, k, off, n)
                    push(ref, ref, ss.at[k], rs.at[k, h, 3], along(ax, d))

        def a4(k):
            for h, _, _ in HALVES:
                landed(line(h, 2, k, 0, hl), rs.at[k, h, 3])

        def drain(k):
            landed(buf.at[:, :, pl.ds(0, hl * 15 // 8)], ss.at[k])

        def a34(k):
            for h in (0, 1):
                for i, d in DIRS + ((2, 2),):
                    landed(line(h, 4 - d, k, 0, hl), rs.at[k, h, 1 + i])

        return (a1, a2, a34, drain) if direct else (a1, a2, a3, a4, drain)

    def base_of(k):
        return k * chunk if isinstance(k, int) else pl.multiple_of(k * chunk, chunk)

    a1, a2, a3, a4, ag_drain = gather_stages(slots, base_of, half, ag_s, ag_r)

    def s0(k):
        if isinstance(k, int):
            landed(slots.at[y, x, pl.ds(0, blk)], own_s.at[0])
            landed(slots.at[y, x, pl.ds(blk, chunk - blk)], dsp_r.at[0])
        else:
            landed(slots.at[y, x, pl.ds(base_of(k), chunk)], dsp_r.at[k])
        a1(k)

    def line(h, d, k, off, n):
        rows = pl.ds(base_of(k) + h * half + off, n)
        if h == 0:
            return part.at[(y + d) % 4, :, rows]
        return part.at[:, (x + d) % 4, rows]

    def one(h, d, k, off, n):
        rows = pl.ds(base_of(k) + h * half + off, n)
        if h == 0:
            return part.at[y, (x + d) % 4, rows]
        return part.at[(y + d) % 4, x, rows]

    SUMS = ((0, "y", "x"), (1, "x", "y"))

    def ffn(k):
        a4(k)

        @pl.when(k == 0)
        def _():
            for copy in loads[6:]:
                copy.wait()

        def norm(b, carry):
            rows = pl.ds(pl.multiple_of(base_of(k) + b * 32, 32), 32)
            total = jnp.zeros((32, 128), F32)
            for t in range(16):
                v = slots[t // 4, t % 4, rows, :].astype(F32)
                total = total + v * v
            inv = lax.rsqrt(jnp.sum(total, axis=1, keepdims=True) / width + EPS)
            put = pl.ds(pl.multiple_of(b * 32, 32), 32)
            for t in range(16):
                v = slots[t // 4, t % 4, rows, :].astype(F32)
                normed[put, t * 128 : (t + 1) * 128] = (
                    v * inv * ffn_gain[:, t * 128 : (t + 1) * 128]
                ).astype(BF16)
            return carry

        lax.fori_loop(0, chunk // 32, norm, 0)
        g = mm(normed[...], gate[...], NT)
        u = mm(normed[...], up[...], NT)
        hidden = (jax.nn.silu(g) * u).astype(BF16)
        rows = pl.ds(base_of(k), chunk)
        for t in range(0, 16, 2):
            p = mm(hidden, down[:, t * 128 : (t + 2) * 128]).astype(BF16)
            part[t // 4, t % 4, rows, :] = p[:, :128]
            part[t // 4, t % 4 + 1, rows, :] = p[:, 128:]
        for h, ax, _ in SUMS:
            for i, d, off, n in pieces(half):
                push(line(h, 2, k, off, n), got1.at[k, h, :, pl.ds(off, n)], rs_s.at[k], rs_r.at[k, h, i], along(ax, d))

    def add(ref, *others):
        total = ref[...].astype(F32)
        for other in others:
            total = total + other[...].astype(F32)
        ref[...] = total.astype(BF16)

    def r2(k):
        for h, ax, _ in SUMS:
            for i, d, off, n in pieces(half):
                landed(got1.at[k, h, :, pl.ds(off, n)], rs_r.at[k, h, i])
                add(line(h, d, k, off, n), got1.at[k, h, :, pl.ds(off, n)])
                push(line(h, d, k, 0, half), got2.at[k, h, i], rs_s.at[k], rs_r.at[k, h, 2], along(ax, d))

    def r3(k):
        for h, _, ax in SUMS:
            landed(got2.at[k, h], rs_r.at[k, h, 2])
            add(line(h, 0, k, 0, half), got2.at[k, h, 0], got2.at[k, h, 1])
            for d in (2, 1, 3):
                push(one(h, d, k, 0, half), got3.at[k, h, d - 1], rs_s.at[k], rs_r.at[k, h, 3], along(ax, d))

    home = pl.ds(pl.multiple_of((z * 2 + c) * blk, blk), blk)

    def back(k):
        for h, _, _ in SUMS:
            landed(got3.at[k, h], rs_r.at[k, h, 3])
            total = one(h, 0, k, 0, half)[...].astype(F32)
            for d in (1, 2, 3):
                total = total + got3[k, h, d - 1].astype(F32)
            summed[pl.ds(base_of(k) + h * half, half), :] = total.astype(BF16)
        for kk in range(NC):

            @pl.when(k == kk)
            def _(kk=kk):
                for i in reversed(range(per)):
                    j = kk * per + i
                    src = summed.at[pl.ds(j * blk, blk)]
                    to = {"z": (z + (DZ[j // 2] + nz) % nz) % nz, "c": (c + j % 2) % 2}
                    if j:
                        push(src, ret.at[home], ret_s, ret_r, to)
                    else:
                        pltpu.make_async_copy(src, ret.at[home], own_s.at[1]).start()

    def rs_drain(k):
        landed(part.at[:, :, pl.ds(0, chunk * 15 // 16)], rs_s.at[k])

    stages = (s0, a2, a3, ffn, r2, r3, back)

    def step(tau, carry):
        for s in ORDER:
            k = tau - s

            @pl.when((k >= 0) & (k < NC))
            def _(s=s, k=k):
                stages[s](k)

        return carry

    s0(0)
    told(4)
    for r in sorted(later, key=lambda r: (r // 4, -abs(DZ[r]))):
        if abs(DZ[r]) > 4:
            dispatch(r, DZ[r])
    fill_selection()
    lax.fori_loop(1, NC + len(stages) - 1, step, 0)

    landed(ret.at[pl.ds(0, blk)], own_s.at[1])
    landed(ret.at[pl.ds(blk, (experts - 1) * blk)], ret_r)
    picked = mm(sel[...], ret[...])
    mix = cols[:, 2:3] * picked[:tokens] + cols[:, 3:4] * picked[tokens:]
    out[y, x, :, :] = (aft[...].astype(F32) + mix).astype(BF16)
    oc = tokens // NO
    *over_out, og_drain = gather_stages(out, lambda k: k * oc, oc // 2, og_s, og_r, True)
    for tau in range(NO + len(over_out) - 1):
        for s, stage in enumerate(over_out):
            if 0 <= tau - s < NO:
                stage(tau - s)
    rim_copy.wait_send()
    landed(sent.at[pl.ds(0, (experts - 1) * blk)], dsp_s)
    landed(summed.at[pl.ds(0, (experts - 1) * blk)], ret_s)

    def drains(k, carry):
        ag_drain(k)
        rs_drain(k)
        return carry

    lax.fori_loop(0, NC, drains, 0)
    for k in range(NO):
        og_drain(k)


def lay_out(src, dst, sem):
    copies = [
        pltpu.make_async_copy(src.at[t // 4, t % 4], dst.at[:, pl.ds(t * 128, 128)], sem.at[t])
        for t in range(16)
    ]
    for copy in copies:
        copy.start()
    for copy in copies:
        copy.wait()


def shards(res, mix_gain, pool_w, pool_scale, ffn_gain, ids, wts, gate, up, down):
    nz = lax.axis_size("z")
    tokens, width = res.shape
    ff = gate.shape[2]
    experts = nz * 2
    blk = tokens * 2 // 16
    total = experts * blk
    chunk = total // NC
    vmem, hbm = pl.BlockSpec(memory_space=pltpu.VMEM), pl.BlockSpec(memory_space=pl.ANY)
    dma, V = pltpu.SemaphoreType.DMA, pltpu.VMEM
    out = pl.pallas_call(
        functools.partial(kernel, nz),
        name="layer",
        out_shape=pltpu.VMEM((4, 4, tokens, 128), BF16),
        in_specs=[hbm] * 10,
        out_specs=vmem,
        scratch_shapes=[
            V((1, width), F32),
            V(pool_w.shape, BF16),
            V((1, 128), F32),
            V((1, width), F32),
            V((2, tokens), jnp.int32),
            V((2, tokens), F32),
            V((tokens, width), BF16),
            V((ff, width), BF16),
            V((ff, width), BF16),
            V((ff, width), BF16),
            V((tokens, width // GROUPS), BF16),
            V((SPAN, width // GROUPS), BF16),
            V((tokens, 128), BF16),
            V((total, tokens), BF16),
            V((experts, tokens), F32),
            V((2 * tokens, total), BF16),
            V((tokens, 8), F32),
            V((total, 128), BF16),
            V((4, 4, total, 128), BF16),
            V((4, 4, total, 128), BF16),
            V((NC, 2, 4, chunk // 2, 128), BF16),
            V((NC, 2, 2, 4, chunk // 2, 128), BF16),
            V((NC, 2, 3, chunk // 2, 128), BF16),
            V((total, 128), BF16),
            V((total, 128), BF16),
            V((chunk, width), BF16),
            dma((10,)),
            dma, dma, dma, dma((NC,)), dma, dma, dma((2,)),
            dma((NC,)), dma((NC, 2, 4)), dma((NC,)), dma((NC, 2, 4)),
            dma((NO,)), dma((NO, 2, 4)),
            pltpu.SemaphoreType.REGULAR((2,)),
        ],
        compiler_params=pltpu.CompilerParams(
            collective_id=0, has_side_effects=True, vmem_limit_bytes=58 * 1024 * 1024
        ),
    )(
        res, mix_gain.reshape(1, -1), pool_w, pool_scale.reshape(1, -1), ffn_gain.reshape(1, -1),
        ids.T, wts.T, gate[0].T, up[0].T, down[0],
    )
    return pl.pallas_call(
        lay_out,
        name="lay_out",
        out_shape=jax.ShapeDtypeStruct((tokens, width), BF16),
        in_specs=[vmem],
        out_specs=hbm,
        scratch_shapes=[dma((16,))],
        compiler_params=pltpu.CompilerParams(vmem_limit_bytes=4 * 1024 * 1024),
    )(out)


def solution(mesh):
    torus = Mesh(mesh.devices.reshape(mesh.shape["sp"] // 2, 2, 4, 4), AXES)
    sp, tp = ("z", "c"), ("y", "x")
    return jax.shard_map(
        shards,
        mesh=torus,
        in_specs=(
            P(sp, None),
            P(),
            P(None, tp),
            P(tp),
            P(),
            P(sp, None),
            P(sp, None),
            P(sp, None, tp),
            P(sp, None, tp),
            P(sp, tp, None),
        ),
        out_specs=P(sp, None),
        check_vma=False,
    )
```
